256 devices in a mesh: ep: 16 (over y, x), tp: 16 (over z, core).
Axes of the slice: x: 4, y: 4, z: 8, core: 2. Of those that a mesh axis runs over, the one named last changes fastest.
Arguments:
- layer_in: bfloat16 [512, 2048], P('ep'), may hold values from -6 to 6
- attn_gain: float32 [2048], replicated, may hold values from 0.1 to 1.9
- query_weight: bfloat16 [2048, 1024], P(None, 'tp'), may hold values from -0.125 to 0.125
- key_weight: bfloat16 [2048, 1024], P(None, 'tp'), may hold values from -0.125 to 0.125
- value_weight: bfloat16 [2048, 1024], P(None, 'tp'), may hold values from -0.125 to 0.125
- forget_weight: bfloat16 [2048, 16], replicated, may hold values from -0.125 to 0.125
- forget_bias: float32 [16], replicated, may hold values from -2 to 3
- out_weight: bfloat16 [1024, 2048], P('tp'), may hold values from -0.1875 to 0.1875
- kv_cache: bfloat16 [512, 16, 1024, 128], P('ep', 'tp'), may hold values from -110 to 110
- cum_gates: float32 [512, 16, 1024], P('ep', 'tp'), may hold values from -144 to 0, as said below
- lengths: int32 [512], P('ep'), may hold values from 512 to 1024, as said below
- ffn_gain: float32 [2048], replicated, may hold values from 0.1 to 1.9
- route_ids: int32 [512, 6], P('ep'), may hold values from 0 to 127, all different within a row; in each aligned block of 32 rows (0 to 31, 32 to 63, ...) at most 2 rows name the same one
- route_weights: float32 [512, 6], P('ep'), may hold values from 0.1 to 1
- shared_gate: bfloat16 [2048, 512], P(None, 'tp'), may hold values from -0.125 to 0.125
- shared_up: bfloat16 [2048, 512], P(None, 'tp'), may hold values from -0.125 to 0.125
- shared_down: bfloat16 [512, 2048], P('tp'), may hold values from -0.25 to 0.25
- expert_gate: bfloat16 [256, 2048, 256], P(('ep', 'tp')), may hold values from -0.125 to 0.125
- expert_up: bfloat16 [256, 2048, 256], P(('ep', 'tp')), may hold values from -0.125 to 0.125
- expert_down: bfloat16 [256, 256, 2048], P(('ep', 'tp')), may hold values from -0.25 to 0.25
Outputs:
- layer_out: bfloat16 [512, 2048], P('ep')
- new_kv: bfloat16 [512, 16, 128], P('ep', 'tp')
The draws below stay inside these ranges and needn't reach their ends.
Inputs may be any that keep to these rules, and one draw needn't show every extreme that they name: `cum_gates`: never rising along positions. `lengths`: every length is at most 1024, and some sequence's length is exactly 1024. `route_ids`: each row names 6 different experts. Among the 32 rows of one index of ep (aligned blocks), no expert is named by more than 2 rows, and in some block one expert is named by exactly 2 rows.
All inputs are finite; a program needn't handle non-finite values.
Results may differ from the reference program's by a relative error of at most 0.019.
Values may be sent and summed in bfloat16 or wider, within the bound.
No kernel may reach another device: no remote copies, remote signals or barrier semaphores. Data moves between devices by JAX's collectives and lax.ppermute only.
A program may use at most 64 MiB of HBM per device.

```python
import math
import jax
import jax.numpy as jnp
import numpy as np
from jax import lax

D = 2048
HEADS = 16
HD = 64
EFF = 512
SFF = 512
TOPK = 6
SEQ_GRP = 32
CACHE_LENGTH = 1024
SEQS = 512
EXPERTS = 128
CAP = 2
N_EP = 16


def draw_kv_cache(key, part):
    tensor_extent = (SEQS, HEADS, CACHE_LENGTH, 2 * HD)
    base = jnp.clip(jax.random.normal(key, tensor_extent, jnp.float32), -6.0, 6.0)
    return base.astype(jnp.bfloat16)


def draw_cum_gates(key, part):
    tensor_extent = (SEQS, HEADS, CACHE_LENGTH)
    slow_share = 0.5
    slow = jax.random.bernoulli(jax.random.fold_in(key, 1), slow_share, (1, HEADS, 1))
    decay_rates = jnp.where(slow, 0.5 / CACHE_LENGTH, 1.0 / 40.0)
    sequence_multiplier = jnp.exp(jax.random.uniform(jax.random.fold_in(key, 2), (SEQS, 1, 1), jnp.float32, -0.7, 0.7))
    approximate_value = jnp.exp(jax.random.uniform(jax.random.fold_in(key, 3), tensor_extent, jnp.float32, -0.7, 0.7))
    spike_position = jax.random.bernoulli(jax.random.fold_in(key, 4), 2.0 / CACHE_LENGTH, tensor_extent)
    spike_length = jax.random.uniform(jax.random.fold_in(key, 5), tensor_extent, jnp.float32, 0.22, 0.69)
    decode_iterations = decay_rates * sequence_multiplier * approximate_value + jnp.where(spike_position, spike_length, 0.0)
    return jnp.cumsum(-decode_iterations, axis=-1)


def draw_lengths(key, part):
    drawn = jax.random.randint(key, (SEQS,), CACHE_LENGTH // 2, CACHE_LENGTH + 1, dtype=jnp.int32)
    return drawn.at[0].set(CACHE_LENGTH)


def block_levels(stream_key, extent, shards, low, top_value):
    def one(dim, shards_of):
        draws = jax.random.uniform(jax.random.fold_in(jax.random.fold_in(stream_key, 6), dim), (shards_of,), jnp.float32, low / len(shards), top_value / len(shards))
        return jnp.repeat(jnp.exp(draws), extent[dim] // shards_of).reshape((-1,) + (1,) * (len(extent) - dim - 1))

    level = one(*shards[0])
    for cut in shards[1:]:
        level = level * one(*cut)
    return level


def deal_out(rng, own, number, rows, amount, top, reach, lean):
    order = jax.random.permutation(rng, amount)
    crowded, ordinary = load_shares(amount, rows * top, reach, lean, True), load_shares(amount, rows * top, reach, lean, False)
    places = jnp.arange(amount)

    def named(sizes, turn):
        used = int((sizes > 0).sum())
        fixed = max(1, used // 4)
        moved = fixed + (places - fixed + turn * (used - fixed)) % max(1, amount - fixed)
        return jnp.zeros((amount,), jnp.int32).at[order[jnp.where(places < fixed, places, moved)]].set(jnp.asarray(sizes, jnp.int32))

    sizes = jnp.where(number % 4 == 0, named(crowded, number // 4), named(ordinary, number - number // 4 - 1))
    mixed = jax.random.permutation(jax.random.fold_in(own, 3), amount)
    donor, receiver = mixed[0:amount // 2 * 2:2], mixed[1:amount // 2 * 2:2]
    margin = jnp.minimum(sizes[donor] - 1, reach - sizes[receiver]) // 2
    margin = jnp.where((donor == order[0]) | (receiver == order[0]) | (sizes[receiver] == 0), 0, jnp.maximum(margin, 0))
    moved = jax.random.randint(jax.random.fold_in(own, 4), (amount // 2,), 0, 1 << 20) % (margin + 1)
    sizes = sizes.at[donor].add(-moved).at[receiver].add(moved)
    items = jnp.searchsorted(jnp.cumsum(sizes), jnp.arange(rows * top), side="right").astype(jnp.int32)
    listing = items.reshape(top, rows).T
    listing = listing[jax.random.permutation(jax.random.fold_in(own, 1), rows)]
    turn = jax.random.randint(jax.random.fold_in(own, 2), (rows, 1), 0, top)
    return jnp.take_along_axis(listing, (jnp.arange(top)[None, :] + turn) % top, axis=1)


def load_shares(amount, total, reach, slope, full):
    portions = [(1 << 20) // math.isqrt(rank ** slope) + 1 for rank in range(1, amount + 1)]
    largest = reach if full else min(reach, max(-(-total // amount), total * portions[0] // sum(portions)))
    least = 1 if total - largest >= amount - 1 else 0
    given, spare = [largest] + [least] * (amount - 1), total - largest - least * (amount - 1)
    while spare > 0:
        free = [i for i in range(1, amount) if given[i] < largest] or [i for i in range(1, amount) if given[i] < reach]
        pool, left = sum([portions[i] for i in free]), spare
        for i in free:
            addition = min(reach - given[i], max(1, left * portions[i] // pool), spare)
            given[i] = given[i] + addition
            spare = spare - addition
    return np.array(given)


def normal_values(stream_key, dims, width, most, cuts=(), kind=jnp.bfloat16):
    entries = jax.random.normal(stream_key, dims, jnp.float32) * width
    if len(cuts) > 0:
        entries = block_levels(stream_key, dims, cuts, -0.22, 0.18) * entries
    return jnp.clip(entries, min=-most, max=most).astype(kind)


def setup_inputs(seed: int = 0) -> dict:
    arg_keys = jax.random.split(jax.random.key(seed), 21)
    layer_in = normal_values(arg_keys[0], (SEQS, D), 1.0, 6.0, ((0, 16),))
    attn_gain = jnp.clip(1.0 + 0.18 * jax.random.normal(arg_keys[1], (D,), jnp.float32), 0.1, 1.9)
    query_weight = normal_values(arg_keys[2], (D, HEADS * HD), D ** -0.5, 0.125, ((1, 16),))
    key_weight = normal_values(arg_keys[3], (D, HEADS * HD), D ** -0.5, 0.125, ((1, 16),))
    value_weight = normal_values(arg_keys[4], (D, HEADS * HD), D ** -0.5, 0.125, ((1, 16),))
    forget_weight = normal_values(arg_keys[5], (D, HEADS), D ** -0.5, 0.125)
    forget_bias = jnp.clip(jax.random.uniform(arg_keys[6], (HEADS,), jnp.float32, -2.0, 3.0), -2.0, 3.0)
    out_weight = normal_values(arg_keys[7], (HEADS * HD, D), (HEADS * HD) ** -0.5, 0.1875, ((0, 16),))
    kv_cache = draw_kv_cache(jax.random.fold_in(arg_keys[20], 71), 0)
    cum_gates = draw_cum_gates(jax.random.fold_in(arg_keys[20], 71), 0)
    lengths = draw_lengths(jax.random.fold_in(arg_keys[20], 71), 0)
    ffn_gain = jnp.clip(1.0 + 0.18 * jax.random.normal(arg_keys[11], (D,), jnp.float32), 0.1, 1.9)
    route_ids_keys = jax.random.split(jax.random.fold_in(arg_keys[12], 1), SEQS // SEQ_GRP)
    route_ids_turns = jax.random.permutation(jax.random.fold_in(arg_keys[12], 3), SEQS // SEQ_GRP)
    route_ids = jax.vmap(lambda own, number: deal_out(jax.random.fold_in(arg_keys[12], 2), own, number, SEQ_GRP, EXPERTS, TOPK, CAP, 2))(route_ids_keys, route_ids_turns).reshape((SEQS, TOPK))
    route_weights = jnp.clip(jnp.exp(math.log(1.0) - 2.3025851 * jax.random.uniform(arg_keys[13], (SEQS, TOPK), jnp.float32) ** block_levels(arg_keys[13], (SEQS, TOPK), ((0, 16),), -0.2, 0.2)), 0.1, 1.0)
    shared_gate = normal_values(arg_keys[14], (D, SFF), D ** -0.5, 0.125, ((1, 16),))
    shared_up = normal_values(arg_keys[15], (D, SFF), D ** -0.5, 0.125, ((1, 16),))
    shared_down = normal_values(arg_keys[16], (SFF, D), SFF ** -0.5, 0.25, ((0, 16),))
    expert_gate = normal_values(arg_keys[17], (2 * EXPERTS, D, EFF // 2), D ** -0.5, 0.125, ((0, 256),))
    expert_up = normal_values(arg_keys[18], (2 * EXPERTS, D, EFF // 2), D ** -0.5, 0.125, ((0, 256),))
    expert_down = normal_values(arg_keys[19], (2 * EXPERTS, EFF // 2, D), EFF ** -0.5, 0.25, ((0, 256),))
    return dict(layer_in=layer_in, attn_gain=attn_gain, query_weight=query_weight, key_weight=key_weight, value_weight=value_weight, forget_weight=forget_weight, forget_bias=forget_bias, out_weight=out_weight, kv_cache=kv_cache, cum_gates=cum_gates, lengths=lengths, ffn_gain=ffn_gain, route_ids=route_ids, route_weights=route_weights, shared_gate=shared_gate, shared_up=shared_up, shared_down=shared_down, expert_gate=expert_gate, expert_up=expert_up, expert_down=expert_down)


NORM_EPS = 1e-06

def rms_scale(stream, gain):
    wide = stream.astype(jnp.float32)
    factor = lax.rsqrt(lax.optimization_barrier(jnp.mean(wide * wide, axis=-1, keepdims=True)) + NORM_EPS)
    return (wide * factor * gain.astype(jnp.float32)).astype(jnp.bfloat16)

def attend(queries, new_key, new_value, forget, kv_block, cum_block, length_block):
    head_size = queries.shape[-1]
    cache_span = kv_block.shape[2]
    positions = jnp.arange(cache_span, dtype=jnp.int32)
    inside = positions[None, None, :] < length_block[:, None, None]
    at_last = positions[None, None, :] == (length_block - 1)[:, None, None]
    latest = lax.optimization_barrier(jnp.sum(jnp.where(at_last, cum_block, 0.0), axis=-1))
    scaling = head_size ** (-0.5)
    cached_keys = kv_block[..., :head_size].astype(jnp.float32)
    cached_values = kv_block[..., head_size:].astype(jnp.float32)
    scores = jnp.einsum('shd,shld->shl', queries.astype(jnp.float32), cached_keys) * scaling
    scores = jnp.where(inside, scores + (latest + forget)[..., None] - cum_block, -jnp.inf)
    itself = lax.optimization_barrier(jnp.sum(queries.astype(jnp.float32) * new_key.astype(jnp.float32), axis=-1)) * scaling
    highest = jnp.maximum(lax.optimization_barrier(jnp.max(scores, axis=-1)), itself)
    earlier = jnp.exp(scores - highest[..., None])
    own_term = jnp.exp(itself - highest)
    denominator = lax.optimization_barrier(jnp.sum(earlier, axis=-1)) + own_term
    past_probs = (earlier / denominator[..., None]).astype(jnp.bfloat16)
    own_probs = (own_term / denominator).astype(jnp.bfloat16)
    blended = jnp.einsum('shl,shld->shd', past_probs.astype(jnp.float32), cached_values)
    blended = blended + own_probs.astype(jnp.float32)[..., None] * new_value.astype(jnp.float32)
    return blended.astype(jnp.bfloat16)

def reference(layer_in, attn_gain, query_weight, key_weight, value_weight, forget_weight, forget_bias, out_weight, kv_cache, cum_gates, lengths, ffn_gain, route_ids, route_weights, shared_gate, shared_up, shared_down, expert_gate, expert_up, expert_down):
    normed = rms_scale(layer_in, attn_gain)
    queries = jnp.dot(normed, query_weight, preferred_element_type=jnp.float32).astype(jnp.bfloat16).reshape(SEQS, HEADS, HD)
    new_key = jnp.dot(normed, key_weight, preferred_element_type=jnp.float32).astype(jnp.bfloat16).reshape(SEQS, HEADS, HD)
    new_value = jnp.dot(normed, value_weight, preferred_element_type=jnp.float32).astype(jnp.bfloat16).reshape(SEQS, HEADS, HD)
    new_kv = jnp.concatenate([new_key, new_value], axis=-1)
    forget = jax.nn.log_sigmoid(jnp.dot(normed, forget_weight, preferred_element_type=jnp.float32) + forget_bias)

    def group_attend(pieces):
        return attend(*pieces)
    attended = lax.map(group_attend, (queries.reshape(N_EP, SEQ_GRP, HEADS, HD), new_key.reshape(N_EP, SEQ_GRP, HEADS, HD), new_value.reshape(N_EP, SEQ_GRP, HEADS, HD), forget.reshape(N_EP, SEQ_GRP, HEADS), kv_cache.reshape(N_EP, SEQ_GRP, HEADS, CACHE_LENGTH, 2 * HD), cum_gates.reshape(N_EP, SEQ_GRP, HEADS, CACHE_LENGTH), lengths.reshape(N_EP, SEQ_GRP)))
    attended = attended.reshape(SEQS, HEADS * HD)
    head_out = jnp.dot(attended, out_weight, preferred_element_type=jnp.float32)
    middle = (layer_in.astype(jnp.float32) + head_out).astype(jnp.bfloat16)
    hidden_in = rms_scale(middle, ffn_gain)
    shared_hidden = (jax.nn.silu(jnp.dot(hidden_in, shared_gate, preferred_element_type=jnp.float32)) * jnp.dot(hidden_in, shared_up, preferred_element_type=jnp.float32)).astype(jnp.bfloat16)
    shared_out = jnp.dot(shared_hidden, shared_down, preferred_element_type=jnp.float32)
    expert_numbers = jnp.arange(EXPERTS, dtype=jnp.int32)
    combine = lax.optimization_barrier(jnp.sum(jnp.where(route_ids[:, :, None] == expert_numbers[None, None, :], route_weights[:, :, None], 0.0), axis=1))
    slot_count = N_EP * CAP
    gate_halves = expert_gate.reshape(EXPERTS, 2, D, EFF // 2)
    up_halves = expert_up.reshape(EXPERTS, 2, D, EFF // 2)
    down_halves = expert_down.reshape(EXPERTS, 2, EFF // 2, D)

    def one_expert(running, pieces):
        gate_half, up_half, down_half, column = pieces
        chosen = column > 0.0
        picked = jnp.nonzero(chosen, size=slot_count, fill_value=0)[0].astype(jnp.int32)
        filled = jnp.arange(slot_count, dtype=jnp.int32) < jnp.sum(chosen.astype(jnp.int32))
        batch_rows = hidden_in[picked]
        gate_full = jnp.concatenate([gate_half[0], gate_half[1]], axis=1)
        up_full = jnp.concatenate([up_half[0], up_half[1]], axis=1)
        down_full = jnp.concatenate([down_half[0], down_half[1]], axis=0)
        hidden = (jax.nn.silu(jnp.dot(batch_rows, gate_full, preferred_element_type=jnp.float32)) * jnp.dot(batch_rows, up_full, preferred_element_type=jnp.float32)).astype(jnp.bfloat16)
        result = jnp.dot(hidden, down_full, preferred_element_type=jnp.float32)
        shares = jnp.where(filled, column[picked], 0.0)
        return (running.at[picked].add(shares[:, None] * result), None)
    routed, _ = lax.scan(one_expert, jnp.zeros((SEQS, D), jnp.float32), (gate_halves, up_halves, down_halves, combine.T))
    layer_out = (middle.astype(jnp.float32) + shared_out + routed).astype(jnp.bfloat16)
    return (layer_out, new_kv)
```

```python
import functools

import jax
import jax.numpy as jnp
from jax import lax
from jax.experimental import pallas as pl
from jax.experimental.pallas import tpu as pltpu
from jax.sharding import Mesh, PartitionSpec as P

NORM_EPS = 1e-06
BF = jnp.bfloat16
F32 = jnp.float32
LANES = 128
VMEM = pltpu.VMEM
EP = ("y", "x")
TP = ("z", "c")
ALL = ("y", "x", "z", "c")


def nt(a, b):
    return lax.dot_general(a, b, (((1,), (1,)), ((), ())), preferred_element_type=F32)


def tn(a, b):
    return lax.dot_general(a, b, (((0,), (0,)), ((), ())), preferred_element_type=F32)


def mm(a, b):
    return jnp.dot(a, b, preferred_element_type=F32)


def rms_rows(wide, gain):
    factor = lax.rsqrt(jnp.mean(wide * wide, axis=-1, keepdims=True) + NORM_EPS)
    return (wide * factor * gain).astype(BF)


def attention_kernel(
    lengths_ref,
    bias_ref,
    head_ref,
    layer_ref,
    gain_ref,
    wq_ref,
    wk_ref,
    wv_ref,
    wf_ref,
    wo_ref,
    cum_ref,
    kv_hbm,
    part_ref,
    newkv_ref,
    kv_buf,
    sems,
):
    rows, width = layer_ref.shape
    span = kv_hbm.shape[2]
    hd = wq_ref.shape[0]
    copies = [
        pltpu.make_async_copy(
            kv_hbm.at[s, 0], kv_buf.at[:, s * LANES : (s + 1) * LANES], sems.at[s]
        )
        for s in range(rows)
    ]
    for copy in copies:
        copy.start()

    normed = rms_rows(layer_ref[...].astype(F32), gain_ref[...])
    padded = jnp.concatenate([normed, jnp.zeros((LANES - rows, width), BF)], axis=0)
    stacked = jnp.concatenate([wq_ref[...], wk_ref[...], wf_ref[...]], axis=0)
    by_seq = nt(stacked, padded)
    query = by_seq[:hd].astype(BF).astype(F32)
    key = by_seq[hd : 2 * hd].astype(BF).astype(F32)
    new_kv = nt(normed, jnp.concatenate([wk_ref[...], wv_ref[...]], axis=0)).astype(BF)
    newkv_ref[...] = new_kv

    scaling = hd ** (-0.5)
    query = query * scaling
    itself = jnp.sum(query * key, axis=0, keepdims=True)
    head = head_ref[0]
    head_row = lax.broadcasted_iota(jnp.int32, (wf_ref.shape[0], LANES), 0) == head
    logit = (
        jnp.sum(jnp.where(head_row, by_seq[2 * hd :], 0.0), axis=0, keepdims=True) + bias_ref[head]
    )
    forget = -(jnp.maximum(-logit, 0.0) + jnp.log1p(jnp.exp(-jnp.abs(logit))))

    lane = lax.broadcasted_iota(jnp.int32, (1, LANES), 1)
    length = jnp.zeros((1, LANES), jnp.int32)
    for s in range(rows):
        length = jnp.where(lane == s, lengths_ref[s], length)

    cum = cum_ref[...].reshape(rows, span)
    cum = jnp.concatenate([cum, jnp.zeros((LANES - rows, span), F32)], axis=0)
    cum = jnp.transpose(cum)
    position = lax.broadcasted_iota(jnp.int32, (span, LANES), 0)
    latest = jnp.sum(jnp.where(position == length - 1, cum, 0.0), axis=0, keepdims=True)
    shift = (latest + forget) - cum

    query = jnp.concatenate([query, jnp.zeros((LANES - hd, LANES), F32)], axis=0)
    lane_full = lax.broadcasted_iota(jnp.int32, (LANES, LANES), 1)
    scores = shift
    group = 8
    for at in range(0, rows, group):
        spread = jnp.concatenate(
            [jnp.where(lane_full == s, query, 0.0).astype(BF) for s in range(at, at + group)],
            axis=0,
        )
        for s in range(at, at + group):
            copies[s].wait()
        scores = scores + mm(kv_buf[:, at * LANES : (at + group) * LANES], spread)

    scores = jnp.where(position < length, scores, -jnp.inf)
    highest = jnp.maximum(jnp.max(scores, axis=0, keepdims=True), itself)
    earlier = jnp.exp(scores - highest)
    own = jnp.exp(itself - highest)
    inverse = 1.0 / (jnp.sum(earlier, axis=0, keepdims=True) + own)
    probs = jnp.transpose(earlier * inverse)[:rows].astype(BF)
    own = (own * inverse).astype(BF).astype(F32)

    square_row = lax.broadcasted_iota(jnp.int32, (rows, LANES), 0)
    square_lane = lax.broadcasted_iota(jnp.int32, (rows, LANES), 1)
    own_column = jnp.sum(
        jnp.where(square_row == square_lane, own, 0.0), axis=1, keepdims=True
    )
    blended = own_column * new_kv.astype(F32)
    for s in range(rows):
        one = mm(probs, kv_buf[:, s * LANES : (s + 1) * LANES])
        blended = blended + jnp.where(square_row == s, one, 0.0)
    attended = blended[:, hd:].astype(BF)
    out = mm(attended, wo_ref[...])
    for t in range(part_ref.shape[0]):
        part_ref[t] = out[:, t * LANES : (t + 1) * LANES].astype(BF)


def route_kernel(ids_ref, weights_ref, place_ref, high_ref, low_ref):
    picks, rows = ids_ref.shape
    many = place_ref.shape[1]
    square = lax.broadcasted_iota(jnp.int32, (rows, rows), 0) == lax.broadcasted_iota(
        jnp.int32, (rows, rows), 1
    )
    slot = lax.broadcasted_iota(jnp.int32, (rows, many), 1)
    row = lax.broadcasted_iota(jnp.int32, (rows, many), 0)
    expert = slot >> 3
    kind = slot & 3
    weight = jnp.zeros((rows, many), F32)
    member = jnp.zeros((rows, many), F32)
    for k in range(picks):
        ids = ids_ref[k : k + 1, :].astype(F32)
        column = jnp.sum(jnp.where(square, ids, 0.0), axis=1, keepdims=True).astype(jnp.int32)
        share = jnp.sum(jnp.where(square, weights_ref[k : k + 1, :], 0.0), axis=1, keepdims=True)
        match = column == expert
        member = jnp.where(match, 1.0, member)
        weight = jnp.where(match, share, weight)
    earlier = (
        lax.broadcasted_iota(jnp.int32, (rows, rows), 0)
        > lax.broadcasted_iota(jnp.int32, (rows, rows), 1)
    )
    ranking = mm(jnp.where(earlier, 1.0, 0.0).astype(BF), member.astype(BF)).astype(jnp.int32)
    routed = jnp.where(ranking == kind, member, 0.0)
    own = jnp.where(row == ((slot >> 6) * 2 + kind - 2), 1.0, 0.0)
    is_routed = kind < 2
    place_ref[...] = jnp.where(is_routed, routed, own).astype(BF)
    shares = jnp.where(is_routed, routed * weight, own)
    high = shares.astype(BF)
    high_ref[...] = high
    low_ref[...] = (shares - high.astype(F32)).astype(BF)


def middle_kernel(tp_ref, arrived_ref, layer_ref, place_ref, middle_ref, send_ref):
    total = arrived_ref[0].astype(F32)
    for t in range(1, arrived_ref.shape[0]):
        total = total + arrived_ref[t].astype(F32)
    start = pl.multiple_of(tp_ref[0] * LANES, LANES)
    middle = (layer_ref[:, pl.ds(start, LANES)].astype(F32) + total).astype(BF)
    middle_ref[...] = middle
    send_ref[...] = tn(place_ref[...], middle).astype(BF)


def expert_kernel(
    arrived_ref,
    gain_ref,
    gate_ref,
    up_ref,
    down_ref,
    sgate_ref,
    sup_ref,
    sdown_ref,
    send_ref,
    wide_ref,
):
    groups = 16
    kinds = 4
    stride = arrived_ref.shape[0] // groups
    tiles = stride // kinds
    wide_ref[...] = arrived_ref[...].astype(F32)

    def rows_of(s):
        return jnp.concatenate(
            [wide_ref[pl.ds(t * kinds + s, groups, stride=stride), :] for t in range(tiles)],
            axis=1,
        )

    def swish(v):
        return v / (1.0 + jnp.exp(-v))

    gain = gain_ref[...]
    routed = rms_rows(jnp.concatenate([rows_of(0), rows_of(1)], axis=0), gain)
    shared = rms_rows(jnp.concatenate([rows_of(2), rows_of(3)], axis=0), gain)
    hidden = (swish(mm(routed, gate_ref[0])) * mm(routed, up_ref[0])).astype(BF)
    served = mm(hidden, down_ref[0])
    shidden = (swish(nt(shared, sgate_ref[...])) * nt(shared, sup_ref[...])).astype(BF)
    sserved = mm(shidden, sdown_ref[...])
    for s, block in enumerate((served, served, sserved, sserved)):
        for t in range(tiles):
            wide_ref[pl.ds(t * kinds + s, groups, stride=stride), :] = block[
                (s % 2) * groups : (s % 2 + 1) * groups, t * LANES : (t + 1) * LANES
            ]
    send_ref[...] = wide_ref[...].astype(BF)


def combine_kernel(arrived_ref, high_ref, low_ref, middle_ref, send_ref):
    arrived = arrived_ref[...]
    total = mm(high_ref[...], arrived) + mm(low_ref[...], arrived)
    out = (middle_ref[...].astype(F32) + total).astype(BF)
    for t in range(send_ref.shape[0]):
        send_ref[t] = out


def exchange(x, axes):
    return lax.all_to_all(x, axes, split_axis=0, concat_axis=0, tiled=True)


def call(kernel, outs, in_specs=None, scratch=(), **more):
    kw = {} if in_specs is None else {"in_specs": in_specs}
    return pl.pallas_call(
        kernel,
        out_shape=outs,
        scratch_shapes=list(scratch),
        **kw,
        **more,
    )


def body(
    layer_in,
    attn_gain,
    query_weight,
    key_weight,
    value_weight,
    forget_weight,
    forget_bias,
    out_weight,
    kv_cache,
    cum_gates,
    lengths,
    ffn_gain,
    route_ids,
    route_weights,
    shared_gate,
    shared_up,
    shared_down,
    expert_gate,
    expert_up,
    expert_down,
):
    rows, width = layer_in.shape
    span = kv_cache.shape[2]
    tp_count = lax.axis_size(TP)
    everyone = lax.axis_size(ALL)
    tp = lax.axis_index(TP).astype(jnp.int32).reshape(1)
    slots = everyone * 4
    shape = jax.ShapeDtypeStruct
    smem = pl.BlockSpec(memory_space=pltpu.SMEM)
    vmem = pl.BlockSpec(memory_space=pltpu.VMEM)
    hbm = pl.BlockSpec(memory_space=pl.ANY)

    place, high, low = call(
        route_kernel, [shape((rows, slots), BF)] * 3, in_specs=[vmem] * 2
    )(route_ids.T, route_weights.T)
    part, new_kv = call(
        attention_kernel,
        [shape((tp_count, rows, LANES), BF), shape((rows, LANES), BF)],
        in_specs=[smem] * 3 + [vmem] * 8 + [hbm],
        scratch=[pltpu.VMEM((span, rows * LANES), BF), pltpu.SemaphoreType.DMA((rows,))],
    )(
        lengths,
        forget_bias,
        tp,
        layer_in,
        attn_gain.reshape(1, width),
        query_weight.T,
        key_weight.T,
        value_weight.T,
        forget_weight.T,
        out_weight,
        cum_gates,
        kv_cache,
    )
    arrived = exchange(part, TP)
    middle, send = call(
        middle_kernel,
        [shape((rows, LANES), BF), shape((slots, LANES), BF)],
        in_specs=[smem] + [vmem] * 3,
    )(tp, arrived, layer_in, place)
    arrived = exchange(send.reshape(everyone, 4, LANES), ALL).reshape(slots, LANES)
    send = call(
        expert_kernel,
        shape((slots, LANES), BF),
        in_specs=[vmem] * 8,
        scratch=[pltpu.VMEM((slots, LANES), F32)],
    )(
        arrived,
        ffn_gain.reshape(1, width),
        expert_gate,
        expert_up,
        expert_down,
        shared_gate.T,
        shared_up.T,
        shared_down,
    )
    arrived = exchange(send.reshape(everyone, 4, LANES), ALL).reshape(slots, LANES)
    send = call(
        combine_kernel, shape((tp_count, rows, LANES), BF), in_specs=[vmem] * 4
    )(arrived, high, low, middle)
    out = exchange(send, TP)
    layer_out = out.transpose(1, 0, 2).reshape(rows, width)
    return (layer_out, new_kv.reshape(rows, 1, LANES))


def solution(mesh):
    split = Mesh(mesh.devices.reshape(4, 4, 8, 2), ALL)
    placed = (
        P(EP, None),
        P(),
        P(None, TP),
        P(None, TP),
        P(None, TP),
        P(),
        P(),
        P(TP, None),
        P(EP, TP, None, None),
        P(EP, TP, None),
        P(EP),
        P(),
        P(EP, None),
        P(EP, None),
        P(None, TP),
        P(None, TP),
        P(TP, None),
        P(ALL, None, None),
        P(ALL, None, None),
        P(ALL, None, None),
    )
    return jax.shard_map(
        body,
        mesh=split,
        in_specs=placed,
        out_specs=(P(EP, None), P(EP, TP, None)),
        check_vma=False,
    )
```

```python
import functools

import jax
import jax.numpy as jnp
from jax import lax
from jax.experimental import pallas as pl
from jax.experimental.pallas import tpu as pltpu
from jax.sharding import Mesh, PartitionSpec as P

NORM_EPS = 1e-06
BF = jnp.bfloat16
F32 = jnp.float32
LANES = 128
VMEM = pltpu.VMEM
EP = ("y", "x")
TP = ("z", "c")
ALL = ("y", "x", "z", "c")


def nt(a, b):
    return lax.dot_general(a, b, (((1,), (1,)), ((), ())), preferred_element_type=F32)


def tn(a, b):
    return lax.dot_general(a, b, (((0,), (0,)), ((), ())), preferred_element_type=F32)


def mm(a, b):
    return jnp.dot(a, b, preferred_element_type=F32)


def rms_rows(wide, gain):
    factor = lax.rsqrt(jnp.mean(wide * wide, axis=-1, keepdims=True) + NORM_EPS)
    return (wide * factor * gain).astype(BF)


def attention_kernel(
    lengths_ref,
    bias_ref,
    head_ref,
    layer_ref,
    gain_ref,
    wq_ref,
    wk_ref,
    wv_ref,
    wf_ref,
    wo_ref,
    cum_ref,
    kv_hbm,
    part_ref,
    newkv_ref,
    kv_buf,
    sems,
):
    rows, width = layer_ref.shape
    span = kv_hbm.shape[2]
    hd = wq_ref.shape[0]
    copies = [
        pltpu.make_async_copy(
            kv_hbm.at[s, 0], kv_buf.at[:, s * LANES : (s + 1) * LANES], sems.at[s]
        )
        for s in range(rows)
    ]
    for copy in copies:
        copy.start()

    normed = rms_rows(layer_ref[...].astype(F32), gain_ref[...])
    padded = jnp.concatenate([normed, jnp.zeros((LANES - rows, width), BF)], axis=0)
    stacked = jnp.concatenate([wq_ref[...], wk_ref[...], wf_ref[...]], axis=0)
    by_seq = nt(stacked, padded)
    query = by_seq[:hd].astype(BF).astype(F32)
    key = by_seq[hd : 2 * hd].astype(BF).astype(F32)
    new_kv = nt(normed, jnp.concatenate([wk_ref[...], wv_ref[...]], axis=0)).astype(BF)
    newkv_ref[...] = new_kv

    scaling = hd ** (-0.5)
    query = query * scaling
    itself = jnp.sum(query * key, axis=0, keepdims=True)
    head = head_ref[0]
    head_row = lax.broadcasted_iota(jnp.int32, (wf_ref.shape[0], LANES), 0) == head
    logit = (
        jnp.sum(jnp.where(head_row, by_seq[2 * hd :], 0.0), axis=0, keepdims=True) + bias_ref[head]
    )
    forget = -(jnp.maximum(-logit, 0.0) + jnp.log1p(jnp.exp(-jnp.abs(logit))))

    lane = lax.broadcasted_iota(jnp.int32, (1, LANES), 1)
    length = jnp.zeros((1, LANES), jnp.int32)
    for s in range(rows):
        length = jnp.where(lane == s, lengths_ref[s], length)

    cum = cum_ref[...].reshape(rows, span)
    cum = jnp.concatenate([cum, jnp.zeros((LANES - rows, span), F32)], axis=0)
    cum = jnp.transpose(cum)
    position = lax.broadcasted_iota(jnp.int32, (span, LANES), 0)
    latest = jnp.sum(jnp.where(position == length - 1, cum, 0.0), axis=0, keepdims=True)
    shift = (latest + forget) - cum

    query = jnp.concatenate([query, jnp.zeros((LANES - hd, LANES), F32)], axis=0)
    lane_full = lax.broadcasted_iota(jnp.int32, (LANES, LANES), 1)
    scores = shift
    group = 8
    for at in range(0, rows, group):
        spread = jnp.concatenate(
            [jnp.where(lane_full == s, query, 0.0).astype(BF) for s in range(at, at + group)],
            axis=0,
        )
        for s in range(at, at + group):
            copies[s].wait()
        scores = scores + mm(kv_buf[:, at * LANES : (at + group) * LANES], spread)

    scores = jnp.where(position < length, scores, -jnp.inf)
    highest = jnp.maximum(jnp.max(scores, axis=0, keepdims=True), itself)
    earlier = jnp.exp(scores - highest)
    own = jnp.exp(itself - highest)
    inverse = 1.0 / (jnp.sum(earlier, axis=0, keepdims=True) + own)
    probs = jnp.transpose(earlier * inverse)[:rows].astype(BF)
    own = (own * inverse).astype(BF).astype(F32)

    square_row = lax.broadcasted_iota(jnp.int32, (rows, LANES), 0)
    square_lane = lax.broadcasted_iota(jnp.int32, (rows, LANES), 1)
    own_column = jnp.sum(
        jnp.where(square_row == square_lane, own, 0.0), axis=1, keepdims=True
    )
    blended = own_column * new_kv.astype(F32)
    for s in range(rows):
        one = mm(probs, kv_buf[:, s * LANES : (s + 1) * LANES])
        blended = blended + jnp.where(square_row == s, one, 0.0)
    attended = blended[:, hd:].astype(BF)
    out = mm(attended, wo_ref[...])
    for t in range(part_ref.shape[0]):
        part_ref[t] = out[:, t * LANES : (t + 1) * LANES].astype(BF)


def route_kernel(ids_ref, weights_ref, place_ref, high_ref, low_ref):
    picks, rows = ids_ref.shape
    many = place_ref.shape[1]
    square = lax.broadcasted_iota(jnp.int32, (rows, rows), 0) == lax.broadcasted_iota(
        jnp.int32, (rows, rows), 1
    )
    slot = lax.broadcasted_iota(jnp.int32, (rows, many), 1)
    row = lax.broadcasted_iota(jnp.int32, (rows, many), 0)
    expert = slot >> 3
    kind = slot & 3
    weight = jnp.zeros((rows, many), F32)
    member = jnp.zeros((rows, many), F32)
    for k in range(picks):
        ids = ids_ref[k : k + 1, :].astype(F32)
        column = jnp.sum(jnp.where(square, ids, 0.0), axis=1, keepdims=True).astype(jnp.int32)
        share = jnp.sum(jnp.where(square, weights_ref[k : k + 1, :], 0.0), axis=1, keepdims=True)
        match = column == expert
        member = jnp.where(match, 1.0, member)
        weight = jnp.where(match, share, weight)
    earlier = (
        lax.broadcasted_iota(jnp.int32, (rows, rows), 0)
        > lax.broadcasted_iota(jnp.int32, (rows, rows), 1)
    )
    ranking = mm(jnp.where(earlier, 1.0, 0.0).astype(BF), member.astype(BF)).astype(jnp.int32)
    routed = jnp.where(ranking == kind, member, 0.0)
    own = jnp.where(row == ((slot >> 6) * 2 + kind - 2), 1.0, 0.0)
    is_routed = kind < 2
    place_ref[...] = jnp.where(is_routed, routed, own).astype(BF)
    shares = jnp.where(is_routed, routed * weight, own)
    high = shares.astype(BF)
    high_ref[...] = high
    low_ref[...] = (shares - high.astype(F32)).astype(BF)


def middle_kernel(tp_ref, arrived_ref, layer_ref, place_ref, middle_ref, send_ref):
    total = arrived_ref[0].astype(F32)
    for t in range(1, arrived_ref.shape[0]):
        total = total + arrived_ref[t].astype(F32)
    start = pl.multiple_of(tp_ref[0] * LANES, LANES)
    middle = (layer_ref[:, pl.ds(start, LANES)].astype(F32) + total).astype(BF)
    middle_ref[...] = middle
    send_ref[...] = tn(place_ref[...], middle).astype(BF)


def expert_kernel(
    arrived_ref,
    gain_ref,
    gate_ref,
    up_ref,
    down_ref,
    sgate_ref,
    sup_ref,
    sdown_ref,
    send_ref,
    wide_ref,
):
    groups = 16
    kinds = 4
    stride = arrived_ref.shape[0] // groups
    tiles = stride // kinds
    wide_ref[...] = arrived_ref[...].astype(F32)

    def rows_of(s):
        return jnp.concatenate(
            [wide_ref[pl.ds(t * kinds + s, groups, stride=stride), :] for t in range(tiles)],
            axis=1,
        )

    def swish(v):
        return v / (1.0 + jnp.exp(-v))

    gain = gain_ref[...]
    routed = rms_rows(jnp.concatenate([rows_of(0), rows_of(1)], axis=0), gain)
    shared = rms_rows(jnp.concatenate([rows_of(2), rows_of(3)], axis=0), gain)
    hidden = (swish(mm(routed, gate_ref[0])) * mm(routed, up_ref[0])).astype(BF)
    served = mm(hidden, down_ref[0])
    shidden = (swish(nt(shared, sgate_ref[...])) * nt(shared, sup_ref[...])).astype(BF)
    sserved = mm(shidden, sdown_ref[...])
    for s, block in enumerate((served, served, sserved, sserved)):
        for t in range(tiles):
            wide_ref[pl.ds(t * kinds + s, groups, stride=stride), :] = block[
                (s % 2) * groups : (s % 2 + 1) * groups, t * LANES : (t + 1) * LANES
            ]
    send_ref[...] = wide_ref[...].astype(BF)


def combine_kernel(arrived_ref, high_ref, low_ref, middle_ref, send_ref):
    arrived = arrived_ref[...]
    total = mm(high_ref[...], arrived) + mm(low_ref[...], arrived)
    out = (middle_ref[...].astype(F32) + total).astype(BF)
    for t in range(send_ref.shape[0]):
        send_ref[t] = out


def exchange(x, axes):
    return lax.all_to_all(x, axes, split_axis=0, concat_axis=0, tiled=True)


def call(kernel, outs, in_specs, scratch=(), limit=16 << 20):
    return pl.pallas_call(
        kernel,
        out_shape=outs,
        in_specs=in_specs,
        scratch_shapes=list(scratch),
        compiler_params=pltpu.CompilerParams(vmem_limit_bytes=limit),
    )


def body(
    layer_in,
    attn_gain,
    query_weight,
    key_weight,
    value_weight,
    forget_weight,
    forget_bias,
    out_weight,
    kv_cache,
    cum_gates,
    lengths,
    ffn_gain,
    route_ids,
    route_weights,
    shared_gate,
    shared_up,
    shared_down,
    expert_gate,
    expert_up,
    expert_down,
):
    rows, width = layer_in.shape
    span = kv_cache.shape[2]
    tp_count = lax.axis_size(TP)
    everyone = lax.axis_size(ALL)
    tp = lax.axis_index(TP).astype(jnp.int32).reshape(1)
    slots = everyone * 4
    shape = jax.ShapeDtypeStruct
    smem = pl.BlockSpec(memory_space=pltpu.SMEM)
    vmem = pl.BlockSpec(memory_space=pltpu.VMEM)
    hbm = pl.BlockSpec(memory_space=pltpu.HBM)

    place, high, low = call(
        route_kernel, [shape((rows, slots), BF)] * 3, in_specs=[vmem] * 2
    )(route_ids.T, route_weights.T)
    part, new_kv = call(
        attention_kernel,
        [shape((tp_count, rows, LANES), BF), shape((rows, LANES), BF)],
        in_specs=[smem] * 3 + [vmem] * 8 + [hbm],
        scratch=[pltpu.VMEM((span, rows * LANES), BF), pltpu.SemaphoreType.DMA((rows,))],
        limit=60 * 1024 * 1024,
    )(
        lengths,
        forget_bias,
        tp,
        layer_in,
        attn_gain.reshape(1, width),
        query_weight.T,
        key_weight.T,
        value_weight.T,
        forget_weight.T,
        out_weight,
        cum_gates,
        kv_cache,
    )
    arrived = exchange(part, TP)
    middle, send = call(
        middle_kernel,
        [shape((rows, LANES), BF), shape((slots, LANES), BF)],
        in_specs=[smem] + [vmem] * 3,
    )(tp, arrived, layer_in, place)
    arrived = exchange(send.reshape(everyone, 4, LANES), ALL).reshape(slots, LANES)
    send = call(
        expert_kernel,
        shape((slots, LANES), BF),
        in_specs=[vmem] * 8,
        scratch=[pltpu.VMEM((slots, LANES), F32)],
    )(
        arrived,
        ffn_gain.reshape(1, width),
        expert_gate,
        expert_up,
        expert_down,
        shared_gate.T,
        shared_up.T,
        shared_down,
    )
    arrived = exchange(send.reshape(everyone, 4, LANES), ALL).reshape(slots, LANES)
    send = call(
        combine_kernel, shape((tp_count, rows, LANES), BF), in_specs=[vmem] * 4
    )(arrived, high, low, middle)
    out = exchange(send, TP)
    layer_out = out.transpose(1, 0, 2).reshape(rows, width)
    return (layer_out, new_kv.reshape(rows, 1, LANES))


def solution(mesh):
    split = Mesh(mesh.devices.reshape(4, 4, 8, 2), ALL)
    placed = (
        P(EP, None),
        P(),
        P(None, TP),
        P(None, TP),
        P(None, TP),
        P(),
        P(),
        P(TP, None),
        P(EP, TP, None, None),
        P(EP, TP, None),
        P(EP),
        P(),
        P(EP, None),
        P(EP, None),
        P(None, TP),
        P(None, TP),
        P(TP, None),
        P(ALL, None, None),
        P(ALL, None, None),
        P(ALL, None, None),
    )
    return jax.shard_map(
        body,
        mesh=split,
        in_specs=placed,
        out_specs=(P(EP, None), P(EP, TP, None)),
        check_vma=False,
    )
```

```python
import functools

import jax
import jax.numpy as jnp
from jax import lax
from jax.experimental import pallas as pl
from jax.experimental.pallas import tpu as pltpu
from jax.sharding import Mesh, PartitionSpec as P

NORM_EPS = 1e-06
BF = jnp.bfloat16
F32 = jnp.float32
LANES = 128
VMEM = pltpu.VMEM
EP = ("y", "x")
TP = ("z", "c")
ALL = ("y", "x", "z", "c")


def nt(a, b):
    return lax.dot_general(a, b, (((1,), (1,)), ((), ())), preferred_element_type=F32)


def tn(a, b):
    return lax.dot_general(a, b, (((0,), (0,)), ((), ())), preferred_element_type=F32)


def mm(a, b):
    return jnp.dot(a, b, preferred_element_type=F32)


def rms_rows(wide, gain):
    factor = lax.rsqrt(jnp.mean(wide * wide, axis=-1, keepdims=True) + NORM_EPS)
    return (wide * factor * gain).astype(BF)


def attention_kernel(
    lengths_hbm,
    bias_hbm,
    head_ref,
    layer_hbm,
    gain_hbm,
    wq_hbm,
    wk_hbm,
    wv_hbm,
    wf_hbm,
    wo_hbm,
    cum_hbm,
    kv_hbm,
    part_ref,
    newkv_ref,
    kv_buf,
    lengths_ref,
    bias_ref,
    layer_ref,
    gain_ref,
    first_ref,
    second_ref,
    wo_ref,
    cum_ref,
    score_ref,
    kv_sems,
    sems,
):
    rows, width = layer_ref.shape
    span = kv_hbm.shape[2]
    hd = wq_hbm.shape[0]
    gates = wf_hbm.shape[0]
    pairs = (
        (layer_hbm, layer_ref),
        (gain_hbm, gain_ref),
        (wq_hbm, first_ref.at[:hd]),
        (wk_hbm, first_ref.at[hd : 2 * hd]),
        (wf_hbm, first_ref.at[2 * hd :]),
        (cum_hbm, cum_ref),
        (wk_hbm, second_ref.at[:hd]),
        (wv_hbm, second_ref.at[hd:]),
        (wo_hbm, wo_ref),
        (lengths_hbm, lengths_ref),
        (bias_hbm, bias_ref),
    )
    small = [pltpu.make_async_copy(a, b, sems.at[i]) for i, (a, b) in enumerate(pairs)]
    group = 8

    def fetch(s):
        at = pl.multiple_of(s * LANES, LANES)
        return pltpu.make_async_copy(kv_hbm.at[s, 0], kv_buf.at[:, pl.ds(at, LANES)], kv_sems.at[s])

    def start(s, carry):
        fetch(s).start()
        return carry

    for copy in small[:6] + small[9:]:
        copy.start()
    lax.fori_loop(0, rows, start, 0)

    for copy in small[:5] + small[9:]:
        copy.wait()
    lane = lax.broadcasted_iota(jnp.int32, (1, LANES), 1)
    length = jnp.zeros((1, LANES), jnp.int32)
    for s in range(rows):
        length = jnp.where(lane == s, lengths_ref[s], length)

    for copy in small[6:9]:
        copy.start()
    normed = rms_rows(layer_ref[...].astype(F32), gain_ref[...])
    padded = jnp.concatenate([normed, jnp.zeros((LANES - rows, width), BF)], axis=0)
    by_seq = nt(first_ref[...], padded)
    query = by_seq[:hd].astype(BF).astype(F32)
    key = by_seq[hd : 2 * hd].astype(BF).astype(F32)

    scaling = hd ** (-0.5)
    query = query * scaling
    itself = jnp.sum(query * key, axis=0, keepdims=True)
    head = head_ref[0]
    head_row = lax.broadcasted_iota(jnp.int32, (gates, LANES), 0) == head
    logit = (
        jnp.sum(jnp.where(head_row, by_seq[2 * hd :], 0.0), axis=0, keepdims=True) + bias_ref[head]
    )
    forget = -(jnp.maximum(-logit, 0.0) + jnp.log1p(jnp.exp(-jnp.abs(logit))))

    small[5].wait()
    cum = cum_ref[...].reshape(rows, span)
    cum = jnp.concatenate([cum, jnp.zeros((LANES - rows, span), F32)], axis=0)
    cum = jnp.transpose(cum)
    position = lax.broadcasted_iota(jnp.int32, (span, LANES), 0)
    latest = jnp.sum(jnp.where(position == length - 1, cum, 0.0), axis=0, keepdims=True)
    shift = (latest + forget) - cum

    query = jnp.concatenate([query, jnp.zeros((LANES - hd, LANES), F32)], axis=0)
    lane_full = lax.broadcasted_iota(jnp.int32, (LANES, LANES), 1)
    score_ref[...] = shift

    def score_step(j, carry):
        first = j * group
        spread = jnp.concatenate(
            [jnp.where(lane_full == first + k, query, 0.0).astype(BF) for k in range(group)],
            axis=0,
        )
        for k in range(group):
            fetch(first + k).wait()
        at = pl.multiple_of(first * LANES, LANES)
        score_ref[...] += mm(kv_buf[:, pl.ds(at, group * LANES)], spread)
        return carry

    lax.fori_loop(0, rows // group, score_step, 0)
    scores = score_ref[...]
    scores = jnp.where(position < length, scores, -jnp.inf)
    highest = jnp.maximum(jnp.max(scores, axis=0, keepdims=True), itself)
    earlier = jnp.exp(scores - highest)
    own = jnp.exp(itself - highest)
    inverse = 1.0 / (jnp.sum(earlier, axis=0, keepdims=True) + own)
    probs = jnp.transpose(earlier * inverse)[:rows].astype(BF)
    own = (own * inverse).astype(BF).astype(F32)

    for copy in small[6:9]:
        copy.wait()
    new_kv = nt(normed, second_ref[...]).astype(BF)
    newkv_ref[...] = new_kv
    square_row = lax.broadcasted_iota(jnp.int32, (rows, LANES), 0)
    square_lane = lax.broadcasted_iota(jnp.int32, (rows, LANES), 1)
    own_column = jnp.sum(
        jnp.where(square_row == square_lane, own, 0.0), axis=1, keepdims=True
    )
    blended = own_column * new_kv.astype(F32)
    step = 8

    def value_step(i, total):
        for k in range(step):
            s = (i * step + k) * 2
            at = pl.multiple_of(s * LANES, LANES)
            two = mm(probs, kv_buf[:, pl.ds(at, 2 * LANES)])
            total = total + jnp.where(square_row == s, two[:, :LANES], 0.0)
            total = total + jnp.where(square_row == s + 1, two[:, LANES:], 0.0)
        return total

    blended = lax.fori_loop(0, rows // (2 * step), value_step, blended)
    attended = blended[:, hd:].astype(BF)
    out = mm(attended, wo_ref[...])
    for t in range(part_ref.shape[0]):
        part_ref[t] = out[:, t * LANES : (t + 1) * LANES].astype(BF)


def routing(ids_ref, weights_ref, many):
    picks, rows = ids_ref.shape
    square = lax.broadcasted_iota(jnp.int32, (rows, rows), 0) == lax.broadcasted_iota(
        jnp.int32, (rows, rows), 1
    )
    slot = lax.broadcasted_iota(jnp.int32, (rows, many), 1)
    row = lax.broadcasted_iota(jnp.int32, (rows, many), 0)
    expert = slot >> 3
    kind = slot & 3
    weight = jnp.zeros((rows, many), F32)
    member = jnp.zeros((rows, many), F32)
    for k in range(picks):
        ids = ids_ref[k : k + 1, :].astype(F32)
        column = jnp.sum(jnp.where(square, ids, 0.0), axis=1, keepdims=True).astype(jnp.int32)
        match = column == expert
        member = jnp.where(match, 1.0, member)
        if weights_ref is not None:
            share = weights_ref[k : k + 1, :]
            share = jnp.sum(jnp.where(square, share, 0.0), axis=1, keepdims=True)
            weight = jnp.where(match, share, weight)
    earlier = (
        lax.broadcasted_iota(jnp.int32, (rows, rows), 0)
        > lax.broadcasted_iota(jnp.int32, (rows, rows), 1)
    )
    ranking = mm(jnp.where(earlier, 1.0, 0.0).astype(BF), member.astype(BF)).astype(jnp.int32)
    routed = jnp.where(ranking == kind, member, 0.0)
    own = jnp.where(row == ((slot >> 6) * 2 + kind - 2), 1.0, 0.0)
    if weights_ref is not None:
        routed = routed * weight
    return jnp.where(kind < 2, routed, own)


def middle_kernel(tp_ref, arrived_ref, layer_ref, ids_ref, middle_ref, send_ref):
    place = routing(ids_ref, None, send_ref.shape[0]).astype(BF)
    total = arrived_ref[0].astype(F32)
    for t in range(1, arrived_ref.shape[0]):
        total = total + arrived_ref[t].astype(F32)
    start = pl.multiple_of(tp_ref[0] * LANES, LANES)
    middle = (layer_ref[:, pl.ds(start, LANES)].astype(F32) + total).astype(BF)
    middle_ref[...] = middle
    send_ref[...] = tn(place, middle).astype(BF)


def expert_kernel(
    arrived_ref,
    gain_ref,
    gate_ref,
    up_ref,
    down_ref,
    sgate_hbm,
    sup_hbm,
    sdown_hbm,
    send_ref,
    wide_ref,
    sgate_ref,
    sup_ref,
    sdown_ref,
    sems,
):
    pairs = ((sgate_hbm, sgate_ref), (sup_hbm, sup_ref), (sdown_hbm, sdown_ref))
    copies = [pltpu.make_async_copy(a, b, sems.at[i]) for i, (a, b) in enumerate(pairs)]
    for copy in copies:
        copy.start()
    groups = 16
    kinds = 4
    stride = arrived_ref.shape[0] // groups
    tiles = stride // kinds
    wide_ref[...] = arrived_ref[...].astype(F32)

    def rows_of(s):
        return jnp.concatenate(
            [wide_ref[pl.ds(t * kinds + s, groups, stride=stride), :] for t in range(tiles)],
            axis=1,
        )

    def swish(v):
        return v / (1.0 + jnp.exp(-v))

    gain = gain_ref[...]
    routed = rms_rows(jnp.concatenate([rows_of(0), rows_of(1)], axis=0), gain)
    shared = rms_rows(jnp.concatenate([rows_of(2), rows_of(3)], axis=0), gain)
    hidden = (swish(mm(routed, gate_ref[0])) * mm(routed, up_ref[0])).astype(BF)
    served = mm(hidden, down_ref[0])
    for copy in copies:
        copy.wait()
    shidden = (swish(nt(shared, sgate_ref[...])) * nt(shared, sup_ref[...])).astype(BF)
    sserved = mm(shidden, sdown_ref[...])
    for s, block in enumerate((served, served, sserved, sserved)):
        for t in range(tiles):
            wide_ref[pl.ds(t * kinds + s, groups, stride=stride), :] = block[
                (s % 2) * groups : (s % 2 + 1) * groups, t * LANES : (t + 1) * LANES
            ]
    send_ref[...] = wide_ref[...].astype(BF)


def combine_kernel(arrived_ref, ids_ref, weights_ref, middle_ref, send_ref):
    shares = routing(ids_ref, weights_ref, arrived_ref.shape[0])
    high = shares.astype(BF)
    low = (shares - high.astype(F32)).astype(BF)
    arrived = arrived_ref[...]
    total = mm(high, arrived) + mm(low, arrived)
    out = (middle_ref[...].astype(F32) + total).astype(BF)
    for t in range(send_ref.shape[0]):
        send_ref[t] = out


def exchange(x, axes):
    return lax.all_to_all(x, axes, split_axis=0, concat_axis=0, tiled=True)


def far(x):
    return pltpu.with_memory_space_constraint(x, pltpu.HBM)


def call(kernel, outs, in_specs, scratch=(), limit=16 << 20):
    return pl.pallas_call(
        kernel,
        out_shape=outs,
        in_specs=in_specs,
        scratch_shapes=list(scratch),
        compiler_params=pltpu.CompilerParams(vmem_limit_bytes=limit),
    )


def body(
    layer_in,
    attn_gain,
    query_weight,
    key_weight,
    value_weight,
    forget_weight,
    forget_bias,
    out_weight,
    kv_cache,
    cum_gates,
    lengths,
    ffn_gain,
    route_ids,
    route_weights,
    shared_gate,
    shared_up,
    shared_down,
    expert_gate,
    expert_up,
    expert_down,
):
    rows, width = layer_in.shape
    span = kv_cache.shape[2]
    hd = query_weight.shape[1]
    gates = forget_weight.shape[1]
    tp_count = lax.axis_size(TP)
    everyone = lax.axis_size(ALL)
    tp = lax.axis_index(TP).astype(jnp.int32).reshape(1)
    slots = everyone * 4
    shape = jax.ShapeDtypeStruct
    smem = pl.BlockSpec(memory_space=pltpu.SMEM)
    vmem = pl.BlockSpec(memory_space=pltpu.VMEM)
    hbm = pl.BlockSpec(memory_space=pltpu.HBM)

    ids = route_ids.T
    part, new_kv = call(
        attention_kernel,
        [shape((tp_count, rows, LANES), BF), shape((rows, LANES), BF)],
        in_specs=[hbm] * 2 + [smem] + [hbm] * 9,
        scratch=[
            VMEM((span, rows * LANES), BF),
            pltpu.SMEM((rows,), jnp.int32),
            pltpu.SMEM((gates,), F32),
            VMEM((rows, width), BF),
            VMEM((1, width), F32),
            VMEM((2 * hd + gates, width), BF),
            VMEM((2 * hd, width), BF),
            VMEM((hd, width), BF),
            VMEM((rows, 1, span), F32),
            VMEM((span, LANES), F32),
            pltpu.SemaphoreType.DMA((rows,)),
            pltpu.SemaphoreType.DMA((11,)),
        ],
        limit=60 * 1024 * 1024,
    )(
        lengths,
        forget_bias,
        tp,
        layer_in,
        attn_gain.reshape(1, width),
        query_weight.T,
        key_weight.T,
        value_weight.T,
        forget_weight.T,
        out_weight,
        cum_gates,
        kv_cache,
    )
    arrived = exchange(part, TP)
    middle, send = call(
        middle_kernel,
        [shape((rows, LANES), BF), shape((slots, LANES), BF)],
        in_specs=[smem] + [vmem] * 3,
    )(tp, arrived, layer_in, ids)
    arrived = exchange(send.reshape(everyone, 4, LANES), ALL).reshape(slots, LANES)
    send = call(
        expert_kernel,
        shape((slots, LANES), BF),
        in_specs=[vmem] * 5 + [hbm] * 3,
        scratch=[VMEM((slots, LANES), F32)]
        + [VMEM((shared_gate.shape[1], width), BF)] * 3
        + [pltpu.SemaphoreType.DMA((3,))],
    )(
        arrived,
        ffn_gain.reshape(1, width),
        expert_gate,
        expert_up,
        expert_down,
        far(shared_gate.T),
        far(shared_up.T),
        far(shared_down),
    )
    arrived = exchange(send.reshape(everyone, 4, LANES), ALL).reshape(slots, LANES)
    send = call(
        combine_kernel, shape((tp_count, rows, LANES), BF), in_specs=[vmem] * 4
    )(arrived, ids, route_weights.T, middle)
    out = exchange(send, TP)
    layer_out = out.transpose(1, 0, 2).reshape(rows, width)
    return (layer_out, new_kv.reshape(rows, 1, LANES))


def solution(mesh):
    split = Mesh(mesh.devices.reshape(4, 4, 8, 2), ALL)
    placed = (
        P(EP, None),
        P(),
        P(None, TP),
        P(None, TP),
        P(None, TP),
        P(),
        P(),
        P(TP, None),
        P(EP, TP, None, None),
        P(EP, TP, None),
        P(EP),
        P(),
        P(EP, None),
        P(EP, None),
        P(None, TP),
        P(None, TP),
        P(TP, None),
        P(ALL, None, None),
        P(ALL, None, None),
        P(ALL, None, None),
    )
    return jax.shard_map(
        body,
        mesh=split,
        in_specs=placed,
        out_specs=(P(EP, None), P(EP, TP, None)),
        check_vma=False,
    )
```

```python
import functools

import jax
import jax.numpy as jnp
from jax import lax
from jax.experimental import pallas as pl
from jax.experimental.pallas import tpu as pltpu
from jax.sharding import Mesh, PartitionSpec as P

NORM_EPS = 1e-06
BF = jnp.bfloat16
F32 = jnp.float32
LANES = 128
VMEM = pltpu.VMEM
EP = ("y", "x")
TP = ("z", "c")
ALL = ("y", "x", "z", "c")


def nt(a, b):
    return lax.dot_general(a, b, (((1,), (1,)), ((), ())), preferred_element_type=F32)


def tn(a, b):
    return lax.dot_general(a, b, (((0,), (0,)), ((), ())), preferred_element_type=F32)


def mm(a, b):
    return jnp.dot(a, b, preferred_element_type=F32)


def rms_rows(wide, gain):
    factor = lax.rsqrt(jnp.mean(wide * wide, axis=-1, keepdims=True) + NORM_EPS)
    return (wide * factor * gain).astype(BF)


def attention_kernel(
    lengths_hbm,
    bias_hbm,
    head_ref,
    layer_hbm,
    gain_hbm,
    wq_hbm,
    wk_hbm,
    wv_hbm,
    wf_hbm,
    wo_hbm,
    cum_hbm,
    kv_hbm,
    part_ref,
    newkv_ref,
    kv_buf,
    lengths_ref,
    bias_ref,
    layer_ref,
    gain_ref,
    first_ref,
    second_ref,
    wo_ref,
    cum_ref,
    score_ref,
    kv_sems,
    sems,
):
    rows, width = layer_ref.shape
    span = kv_hbm.shape[2]
    hd = wq_hbm.shape[0]
    gates = wf_hbm.shape[0]
    pairs = (
        (layer_hbm, layer_ref),
        (gain_hbm, gain_ref),
        (wq_hbm, first_ref.at[:hd]),
        (wk_hbm, first_ref.at[hd : 2 * hd]),
        (wf_hbm, first_ref.at[2 * hd :]),
        (cum_hbm, cum_ref),
        (wk_hbm, second_ref.at[:hd]),
        (wv_hbm, second_ref.at[hd:]),
        (wo_hbm, wo_ref),
        (lengths_hbm, lengths_ref),
        (bias_hbm, bias_ref),
    )
    small = [pltpu.make_async_copy(a, b, sems.at[i]) for i, (a, b) in enumerate(pairs)]
    group = 8

    def fetch(s):
        at = pl.multiple_of(s * LANES, LANES)
        return pltpu.make_async_copy(kv_hbm.at[s, 0], kv_buf.at[:, pl.ds(at, LANES)], kv_sems.at[s])

    def start(s, carry):
        fetch(s).start()
        return carry

    for copy in small:
        copy.start()
    lax.fori_loop(0, rows, start, 0)

    for copy in small[:5] + small[9:]:
        copy.wait()
    lane = lax.broadcasted_iota(jnp.int32, (1, LANES), 1)
    length = jnp.zeros((1, LANES), jnp.int32)
    for s in range(rows):
        length = jnp.where(lane == s, lengths_ref[s], length)

    normed = rms_rows(layer_ref[...].astype(F32), gain_ref[...])
    padded = jnp.concatenate([normed, jnp.zeros((LANES - rows, width), BF)], axis=0)
    by_seq = nt(first_ref[...], padded)
    query = by_seq[:hd].astype(BF).astype(F32)
    key = by_seq[hd : 2 * hd].astype(BF).astype(F32)

    scaling = hd ** (-0.5)
    query = query * scaling
    itself = jnp.sum(query * key, axis=0, keepdims=True)
    head = head_ref[0]
    head_row = lax.broadcasted_iota(jnp.int32, (gates, LANES), 0) == head
    logit = (
        jnp.sum(jnp.where(head_row, by_seq[2 * hd :], 0.0), axis=0, keepdims=True) + bias_ref[head]
    )
    forget = -(jnp.maximum(-logit, 0.0) + jnp.log1p(jnp.exp(-jnp.abs(logit))))

    small[5].wait()
    cum = cum_ref[...].reshape(rows, span)
    cum = jnp.concatenate([cum, jnp.zeros((LANES - rows, span), F32)], axis=0)
    cum = jnp.transpose(cum)
    position = lax.broadcasted_iota(jnp.int32, (span, LANES), 0)
    latest = jnp.sum(jnp.where(position == length - 1, cum, 0.0), axis=0, keepdims=True)
    shift = (latest + forget) - cum

    for copy in small[6:9]:
        copy.wait()
    new_kv = nt(normed, second_ref[...]).astype(BF)
    newkv_ref[...] = new_kv
    query = jnp.concatenate([query, jnp.zeros((LANES - hd, LANES), F32)], axis=0)
    lane_full = lax.broadcasted_iota(jnp.int32, (LANES, LANES), 1)
    score_ref[...] = shift

    def score_step(j, carry):
        first = j * group
        spread = jnp.concatenate(
            [jnp.where(lane_full == first + k, query, 0.0).astype(BF) for k in range(group)],
            axis=0,
        )
        for k in range(group):
            fetch(first + k).wait()
        at = pl.multiple_of(first * LANES, LANES)
        score_ref[...] += mm(kv_buf[:, pl.ds(at, group * LANES)], spread)
        return carry

    lax.fori_loop(0, rows // group, score_step, 0)
    scores = score_ref[...]
    scores = jnp.where(position < length, scores, -jnp.inf)
    highest = jnp.maximum(jnp.max(scores, axis=0, keepdims=True), itself)
    earlier = jnp.exp(scores - highest)
    own = jnp.exp(itself - highest)
    inverse = 1.0 / (jnp.sum(earlier, axis=0, keepdims=True) + own)
    probs = jnp.transpose(earlier * inverse)[:rows].astype(BF)
    own = (own * inverse).astype(BF).astype(F32)

    square_row = lax.broadcasted_iota(jnp.int32, (rows, LANES), 0)
    square_lane = lax.broadcasted_iota(jnp.int32, (rows, LANES), 1)
    own_column = jnp.sum(
        jnp.where(square_row == square_lane, own, 0.0), axis=1, keepdims=True
    )
    blended = own_column * new_kv.astype(F32)
    step = 16

    def value_step(i, total):
        for k in range(step):
            s = (i * step + k) * 2
            at = pl.multiple_of(s * LANES, LANES)
            two = mm(probs, kv_buf[:, pl.ds(at, 2 * LANES)])
            total = total + jnp.where(square_row == s, two[:, :LANES], 0.0)
            total = total + jnp.where(square_row == s + 1, two[:, LANES:], 0.0)
        return total

    blended = lax.fori_loop(0, rows // (2 * step), value_step, blended)
    attended = blended[:, hd:].astype(BF)
    out = mm(attended, wo_ref[...])
    for t in range(part_ref.shape[0]):
        part_ref[t] = out[:, t * LANES : (t + 1) * LANES].astype(BF)


def routing(ids_ref, weights_ref, many):
    picks, rows = ids_ref.shape
    square = lax.broadcasted_iota(jnp.int32, (rows, rows), 0) == lax.broadcasted_iota(
        jnp.int32, (rows, rows), 1
    )
    slot = lax.broadcasted_iota(jnp.int32, (rows, many), 1)
    row = lax.broadcasted_iota(jnp.int32, (rows, many), 0)
    expert = slot >> 3
    kind = slot & 3
    weight = jnp.zeros((rows, many), F32)
    member = jnp.zeros((rows, many), F32)
    for k in range(picks):
        ids = ids_ref[k : k + 1, :].astype(F32)
        column = jnp.sum(jnp.where(square, ids, 0.0), axis=1, keepdims=True).astype(jnp.int32)
        match = column == expert
        member = jnp.where(match, 1.0, member)
        if weights_ref is not None:
            share = weights_ref[k : k + 1, :]
            share = jnp.sum(jnp.where(square, share, 0.0), axis=1, keepdims=True)
            weight = jnp.where(match, share, weight)
    earlier = (
        lax.broadcasted_iota(jnp.int32, (rows, rows), 0)
        > lax.broadcasted_iota(jnp.int32, (rows, rows), 1)
    )
    ranking = mm(jnp.where(earlier, 1.0, 0.0).astype(BF), member.astype(BF)).astype(jnp.int32)
    routed = jnp.where(ranking == kind, member, 0.0)
    own = jnp.where(row == ((slot >> 6) * 2 + kind - 2), 1.0, 0.0)
    if weights_ref is not None:
        routed = routed * weight
    return jnp.where(kind < 2, routed, own)


def middle_kernel(tp_ref, arrived_ref, layer_ref, ids_ref, middle_ref, send_ref):
    place = routing(ids_ref, None, send_ref.shape[0]).astype(BF)
    total = arrived_ref[0].astype(F32)
    for t in range(1, arrived_ref.shape[0]):
        total = total + arrived_ref[t].astype(F32)
    start = pl.multiple_of(tp_ref[0] * LANES, LANES)
    middle = (layer_ref[:, pl.ds(start, LANES)].astype(F32) + total).astype(BF)
    middle_ref[...] = middle
    send_ref[...] = tn(place, middle).astype(BF)


def expert_kernel(
    arrived_ref,
    gain_ref,
    gate_ref,
    up_ref,
    down_ref,
    sgate_ref,
    sup_ref,
    sdown_hbm,
    send_ref,
    wide_ref,
    sdown_ref,
    sem,
):
    copy = pltpu.make_async_copy(sdown_hbm, sdown_ref, sem)
    copy.start()
    groups = 16
    kinds = 4
    stride = arrived_ref.shape[0] // groups
    tiles = stride // kinds
    wide_ref[...] = arrived_ref[...].astype(F32)

    def rows_of(s):
        return jnp.concatenate(
            [wide_ref[pl.ds(t * kinds + s, groups, stride=stride), :] for t in range(tiles)],
            axis=1,
        )

    def swish(v):
        return v / (1.0 + jnp.exp(-v))

    gain = gain_ref[...]
    routed = rms_rows(jnp.concatenate([rows_of(0), rows_of(1)], axis=0), gain)
    shared = rms_rows(jnp.concatenate([rows_of(2), rows_of(3)], axis=0), gain)
    hidden = (swish(mm(routed, gate_ref[0])) * mm(routed, up_ref[0])).astype(BF)
    served = mm(hidden, down_ref[0])
    shidden = (swish(nt(shared, sgate_ref[...])) * nt(shared, sup_ref[...])).astype(BF)
    copy.wait()
    sserved = mm(shidden, sdown_ref[...])
    for s, block in enumerate((served, served, sserved, sserved)):
        for t in range(tiles):
            wide_ref[pl.ds(t * kinds + s, groups, stride=stride), :] = block[
                (s % 2) * groups : (s % 2 + 1) * groups, t * LANES : (t + 1) * LANES
            ]
    send_ref[...] = wide_ref[...].astype(BF)


def combine_kernel(arrived_ref, ids_ref, weights_ref, middle_ref, send_ref):
    shares = routing(ids_ref, weights_ref, arrived_ref.shape[0])
    high = shares.astype(BF)
    low = (shares - high.astype(F32)).astype(BF)
    arrived = arrived_ref[...]
    total = mm(high, arrived) + mm(low, arrived)
    out = (middle_ref[...].astype(F32) + total).astype(BF)
    for t in range(send_ref.shape[0]):
        send_ref[t] = out


def exchange(x, axes):
    return lax.all_to_all(x, axes, split_axis=0, concat_axis=0, tiled=True)


def far(x):
    return pltpu.with_memory_space_constraint(x, pltpu.HBM)


def call(kernel, outs, in_specs, scratch=(), limit=16 << 20):
    return pl.pallas_call(
        kernel,
        out_shape=outs,
        in_specs=in_specs,
        scratch_shapes=list(scratch),
        compiler_params=pltpu.CompilerParams(vmem_limit_bytes=limit),
    )


def body(
    layer_in,
    attn_gain,
    query_weight,
    key_weight,
    value_weight,
    forget_weight,
    forget_bias,
    out_weight,
    kv_cache,
    cum_gates,
    lengths,
    ffn_gain,
    route_ids,
    route_weights,
    shared_gate,
    shared_up,
    shared_down,
    expert_gate,
    expert_up,
    expert_down,
):
    rows, width = layer_in.shape
    span = kv_cache.shape[2]
    hd = query_weight.shape[1]
    gates = forget_weight.shape[1]
    tp_count = lax.axis_size(TP)
    everyone = lax.axis_size(ALL)
    tp = lax.axis_index(TP).astype(jnp.int32).reshape(1)
    slots = everyone * 4
    shape = jax.ShapeDtypeStruct
    smem = pl.BlockSpec(memory_space=pltpu.SMEM)
    vmem = pl.BlockSpec(memory_space=pltpu.VMEM)
    hbm = pl.BlockSpec(memory_space=pltpu.HBM)

    ids = route_ids.T
    part, new_kv = call(
        attention_kernel,
        [shape((tp_count, rows, LANES), BF), shape((rows, LANES), BF)],
        in_specs=[hbm] * 2 + [smem] + [hbm] * 9,
        scratch=[
            VMEM((span, rows * LANES), BF),
            pltpu.SMEM((rows,), jnp.int32),
            pltpu.SMEM((gates,), F32),
            VMEM((rows, width), BF),
            VMEM((1, width), F32),
            VMEM((2 * hd + gates, width), BF),
            VMEM((2 * hd, width), BF),
            VMEM((hd, width), BF),
            VMEM((rows, 1, span), F32),
            VMEM((span, LANES), F32),
            pltpu.SemaphoreType.DMA((rows,)),
            pltpu.SemaphoreType.DMA((11,)),
        ],
        limit=24 << 20,
    )(
        far(lengths),
        far(forget_bias),
        tp,
        far(layer_in),
        far(attn_gain.reshape(1, width)),
        far(query_weight.T),
        far(key_weight.T),
        far(value_weight.T),
        far(forget_weight.T),
        far(out_weight),
        far(cum_gates),
        far(kv_cache),
    )
    arrived = exchange(part, TP)
    middle, send = call(
        middle_kernel,
        [shape((rows, LANES), BF), shape((slots, LANES), BF)],
        in_specs=[smem] + [vmem] * 3,
    )(tp, arrived, layer_in, ids)
    arrived = exchange(send.reshape(everyone, 4, LANES), ALL).reshape(slots, LANES)
    send = call(
        expert_kernel,
        shape((slots, LANES), BF),
        in_specs=[vmem] * 7 + [hbm],
        scratch=[
            VMEM((slots, LANES), F32),
            VMEM(shared_down.shape, BF),
            pltpu.SemaphoreType.DMA,
        ],
    )(
        arrived,
        ffn_gain.reshape(1, width),
        expert_gate,
        expert_up,
        expert_down,
        shared_gate.T,
        shared_up.T,
        far(shared_down),
    )
    arrived = exchange(send.reshape(everyone, 4, LANES), ALL).reshape(slots, LANES)
    send = call(
        combine_kernel, shape((tp_count, rows, LANES), BF), in_specs=[vmem] * 4
    )(arrived, ids, route_weights.T, middle)
    out = exchange(send, TP)
    layer_out = out.transpose(1, 0, 2).reshape(rows, width)
    return (layer_out, new_kv.reshape(rows, 1, LANES))


def solution(mesh):
    split = Mesh(mesh.devices.reshape(4, 4, 8, 2), ALL)
    placed = (
        P(EP, None),
        P(),
        P(None, TP),
        P(None, TP),
        P(None, TP),
        P(),
        P(),
        P(TP, None),
        P(EP, TP, None, None),
        P(EP, TP, None),
        P(EP),
        P(),
        P(EP, None),
        P(EP, None),
        P(None, TP),
        P(None, TP),
        P(TP, None),
        P(ALL, None, None),
        P(ALL, None, None),
        P(ALL, None, None),
    )
    return jax.shard_map(
        body,
        mesh=split,
        in_specs=placed,
        out_specs=(P(EP, None), P(EP, TP, None)),
        check_vma=False,
    )
```

```python
import functools

import jax
import jax.numpy as jnp
from jax import lax
from jax.experimental import pallas as pl
from jax.experimental.pallas import tpu as pltpu
from jax.sharding import Mesh, PartitionSpec as P

NORM_EPS = 1e-06
BF = jnp.bfloat16
F32 = jnp.float32
LANES = 128
VMEM = pltpu.VMEM
EP = ("y", "x")
TP = ("z", "c")
ALL = ("y", "x", "z", "c")
CHIPS = ("y", "x", "z")
SWAP = ((0, 1), (1, 0))


def nt(a, b):
    return lax.dot_general(a, b, (((1,), (1,)), ((), ())), preferred_element_type=F32)


def tn(a, b):
    return lax.dot_general(a, b, (((0,), (0,)), ((), ())), preferred_element_type=F32)


def mm(a, b):
    return jnp.dot(a, b, preferred_element_type=F32)


def rms_rows(wide, gain):
    factor = lax.rsqrt(jnp.mean(wide * wide, axis=-1, keepdims=True) + NORM_EPS)
    return (wide * factor * gain).astype(BF)


def attention_kernel(
    lengths_hbm,
    bias_hbm,
    head_ref,
    layer_hbm,
    gain_hbm,
    wq_hbm,
    wk_hbm,
    wv_hbm,
    wf_hbm,
    wo_hbm,
    cum_hbm,
    kv_hbm,
    part_ref,
    newkv_ref,
    kv_buf,
    lengths_ref,
    bias_ref,
    layer_ref,
    gain_ref,
    first_ref,
    second_ref,
    wo_ref,
    cum_ref,
    score_ref,
    kv_sems,
    sems,
):
    rows, width = layer_ref.shape
    span = kv_hbm.shape[2]
    hd = wq_hbm.shape[0]
    gates = wf_hbm.shape[0]
    pairs = (
        (layer_hbm, layer_ref),
        (gain_hbm, gain_ref),
        (wq_hbm, first_ref.at[:hd]),
        (wk_hbm, first_ref.at[hd : 2 * hd]),
        (wf_hbm, first_ref.at[2 * hd :]),
        (cum_hbm, cum_ref),
        (wk_hbm, second_ref.at[:hd]),
        (wv_hbm, second_ref.at[hd:]),
        (wo_hbm, wo_ref),
        (lengths_hbm, lengths_ref),
        (bias_hbm, bias_ref),
    )
    small = [pltpu.make_async_copy(a, b, sems.at[i]) for i, (a, b) in enumerate(pairs)]
    group = 8

    def fetch(s):
        at = pl.multiple_of(s * LANES, LANES)
        return pltpu.make_async_copy(kv_hbm.at[s, 0], kv_buf.at[:, pl.ds(at, LANES)], kv_sems.at[s])

    def start(s, carry):
        fetch(s).start()
        return carry

    for copy in small:
        copy.start()
    lax.fori_loop(0, rows, start, 0)

    for copy in small[:5] + small[9:]:
        copy.wait()
    lane = lax.broadcasted_iota(jnp.int32, (1, LANES), 1)
    length = jnp.zeros((1, LANES), jnp.int32)
    for s in range(rows):
        length = jnp.where(lane == s, lengths_ref[s], length)

    normed = rms_rows(layer_ref[...].astype(F32), gain_ref[...])
    padded = jnp.concatenate([normed, jnp.zeros((LANES - rows, width), BF)], axis=0)
    by_seq = nt(first_ref[...], padded)
    query = by_seq[:hd].astype(BF).astype(F32)
    key = by_seq[hd : 2 * hd].astype(BF).astype(F32)

    scaling = hd ** (-0.5)
    query = query * scaling
    itself = jnp.sum(query * key, axis=0, keepdims=True)
    head = head_ref[0]
    head_row = lax.broadcasted_iota(jnp.int32, (gates, LANES), 0) == head
    logit = (
        jnp.sum(jnp.where(head_row, by_seq[2 * hd :], 0.0), axis=0, keepdims=True) + bias_ref[head]
    )
    forget = -(jnp.maximum(-logit, 0.0) + jnp.log1p(jnp.exp(-jnp.abs(logit))))

    small[5].wait()
    cum = cum_ref[...].reshape(rows, span)
    cum = jnp.concatenate([cum, jnp.zeros((LANES - rows, span), F32)], axis=0)
    cum = jnp.transpose(cum)
    position = lax.broadcasted_iota(jnp.int32, (span, LANES), 0)
    latest = jnp.sum(jnp.where(position == length - 1, cum, 0.0), axis=0, keepdims=True)
    shift = (latest + forget) - cum

    for copy in small[6:9]:
        copy.wait()
    new_kv = nt(normed, second_ref[...]).astype(BF)
    newkv_ref[...] = new_kv
    query = jnp.concatenate([query, jnp.zeros((LANES - hd, LANES), F32)], axis=0)
    lane_full = lax.broadcasted_iota(jnp.int32, (LANES, LANES), 1)
    score_ref[...] = shift

    def score_step(j, carry):
        first = j * group
        spread = jnp.concatenate(
            [jnp.where(lane_full == first + k, query, 0.0).astype(BF) for k in range(group)],
            axis=0,
        )
        for k in range(group):
            fetch(first + k).wait()
        at = pl.multiple_of(first * LANES, LANES)
        score_ref[...] += mm(kv_buf[:, pl.ds(at, group * LANES)], spread)
        return carry

    lax.fori_loop(0, rows // group, score_step, 0)
    scores = score_ref[...]
    scores = jnp.where(position < length, scores, -jnp.inf)
    highest = jnp.maximum(jnp.max(scores, axis=0, keepdims=True), itself)
    earlier = jnp.exp(scores - highest)
    own = jnp.exp(itself - highest)
    inverse = 1.0 / (jnp.sum(earlier, axis=0, keepdims=True) + own)
    probs = jnp.transpose(earlier * inverse)[:rows].astype(BF)
    own = (own * inverse).astype(BF).astype(F32)

    square_row = lax.broadcasted_iota(jnp.int32, (rows, LANES), 0)
    square_lane = lax.broadcasted_iota(jnp.int32, (rows, LANES), 1)
    own_column = jnp.sum(
        jnp.where(square_row == square_lane, own, 0.0), axis=1, keepdims=True
    )
    blended = own_column * new_kv.astype(F32)
    step = 16

    def value_step(i, total):
        for k in range(step):
            s = (i * step + k) * 2
            at = pl.multiple_of(s * LANES, LANES)
            two = mm(probs, kv_buf[:, pl.ds(at, 2 * LANES)])
            total = total + jnp.where(square_row == s, two[:, :LANES], 0.0)
            total = total + jnp.where(square_row == s + 1, two[:, LANES:], 0.0)
        return total

    blended = lax.fori_loop(0, rows // (2 * step), value_step, blended)
    attended = blended[:, hd:].astype(BF)
    out = mm(attended, wo_ref[...])
    for t in range(part_ref.shape[0]):
        part_ref[t] = out[:, t * LANES : (t + 1) * LANES].astype(BF)


def routing(ids_ref, weights_ref, many):
    picks, rows = ids_ref.shape
    square = lax.broadcasted_iota(jnp.int32, (rows, rows), 0) == lax.broadcasted_iota(
        jnp.int32, (rows, rows), 1
    )
    slot = lax.broadcasted_iota(jnp.int32, (rows, many), 1)
    row = lax.broadcasted_iota(jnp.int32, (rows, many), 0)
    expert = slot >> 2
    kind = slot & 3
    weight = jnp.zeros((rows, many), F32)
    member = jnp.zeros((rows, many), F32)
    for k in range(picks):
        ids = ids_ref[k : k + 1, :].astype(F32)
        column = jnp.sum(jnp.where(square, ids, 0.0), axis=1, keepdims=True).astype(jnp.int32)
        match = column == expert
        member = jnp.where(match, 1.0, member)
        if weights_ref is not None:
            share = weights_ref[k : k + 1, :]
            share = jnp.sum(jnp.where(square, share, 0.0), axis=1, keepdims=True)
            weight = jnp.where(match, share, weight)
    earlier = (
        lax.broadcasted_iota(jnp.int32, (rows, rows), 0)
        > lax.broadcasted_iota(jnp.int32, (rows, rows), 1)
    )
    ranking = mm(jnp.where(earlier, 1.0, 0.0).astype(BF), member.astype(BF)).astype(jnp.int32)
    routed = jnp.where(ranking == kind, member, 0.0)
    own = jnp.where(row == ((slot >> 5) * 2 + kind - 2), 1.0, 0.0)
    if weights_ref is not None:
        routed = routed * weight
    return jnp.where(kind < 2, routed, own)


def middle_kernel(tp_ref, arrived_ref, layer_ref, ids_ref, middle_ref, send_ref):
    place = routing(ids_ref, None, send_ref.shape[0]).astype(BF)
    total = arrived_ref[0].astype(F32)
    for t in range(1, arrived_ref.shape[0]):
        total = total + arrived_ref[t].astype(F32)
    start = pl.multiple_of(tp_ref[0] * LANES, LANES)
    middle = (layer_ref[:, pl.ds(start, LANES)].astype(F32) + total).astype(BF)
    middle_ref[...] = middle
    send_ref[...] = tn(place, middle).astype(BF)


def expert_kernel(
    core_ref,
    mine_ref,
    theirs_ref,
    gain_ref,
    gate_ref,
    up_ref,
    down_ref,
    sgate_ref,
    sup_ref,
    sdown_hbm,
    keep_ref,
    give_ref,
    even_ref,
    odd_ref,
    sdown_ref,
    sem,
):
    copy = pltpu.make_async_copy(sdown_hbm, sdown_ref, sem)
    copy.start()
    groups = 16
    kinds = 4
    stride = mine_ref.shape[0] // groups
    tiles = stride // kinds
    first = core_ref[0] == 0
    mine = mine_ref[...].astype(F32)
    theirs = theirs_ref[...].astype(F32)
    even_ref[...] = jnp.where(first, mine, theirs)
    odd_ref[...] = jnp.where(first, theirs, mine)
    sides = (even_ref, odd_ref)

    def rows_of(s):
        return jnp.concatenate(
            [
                sides[t % 2][pl.ds((t // 2) * kinds + s, groups, stride=stride), :]
                for t in range(2 * tiles)
            ],
            axis=1,
        )

    def swish(v):
        return v / (1.0 + jnp.exp(-v))

    gain = gain_ref[...]
    routed = rms_rows(jnp.concatenate([rows_of(0), rows_of(1)], axis=0), gain)
    shared = rms_rows(jnp.concatenate([rows_of(2), rows_of(3)], axis=0), gain)
    hidden = (swish(mm(routed, gate_ref[0])) * mm(routed, up_ref[0])).astype(BF)
    served = mm(hidden, down_ref[0])
    shidden = (swish(nt(shared, sgate_ref[...])) * nt(shared, sup_ref[...])).astype(BF)
    copy.wait()
    sserved = mm(shidden, sdown_ref[...])
    for s, block in enumerate((served, served, sserved, sserved)):
        for t in range(2 * tiles):
            sides[t % 2][pl.ds((t // 2) * kinds + s, groups, stride=stride), :] = block[
                (s % 2) * groups : (s % 2 + 1) * groups, t * LANES : (t + 1) * LANES
            ]
    even = even_ref[...]
    odd = odd_ref[...]
    keep_ref[...] = jnp.where(first, even, odd)
    give_ref[...] = jnp.where(first, odd, even).astype(BF)


def combine_kernel(arrived_ref, ids_ref, weights_ref, middle_ref, send_ref):
    shares = routing(ids_ref, weights_ref, arrived_ref.shape[0])
    high = shares.astype(BF)
    low = (shares - high.astype(F32)).astype(BF)
    arrived = arrived_ref[...]
    total = mm(high, arrived) + mm(low, arrived)
    out = (middle_ref[...].astype(F32) + total).astype(BF)
    for t in range(send_ref.shape[0]):
        send_ref[t] = out


def exchange(x, axes):
    return lax.all_to_all(x, axes, split_axis=0, concat_axis=0, tiled=True)


def far(x):
    return pltpu.with_memory_space_constraint(x, pltpu.HBM)


def call(kernel, outs, in_specs, scratch=(), limit=16 << 20):
    return pl.pallas_call(
        kernel,
        out_shape=outs,
        in_specs=in_specs,
        scratch_shapes=list(scratch),
        compiler_params=pltpu.CompilerParams(vmem_limit_bytes=limit),
    )


def body(
    layer_in,
    attn_gain,
    query_weight,
    key_weight,
    value_weight,
    forget_weight,
    forget_bias,
    out_weight,
    kv_cache,
    cum_gates,
    lengths,
    ffn_gain,
    route_ids,
    route_weights,
    shared_gate,
    shared_up,
    shared_down,
    expert_gate,
    expert_up,
    expert_down,
):
    rows, width = layer_in.shape
    span = kv_cache.shape[2]
    hd = query_weight.shape[1]
    gates = forget_weight.shape[1]
    tp_count = lax.axis_size(TP)
    chips = lax.axis_size(CHIPS)
    core = lax.axis_index("c").astype(jnp.int32).reshape(1)
    tp = lax.axis_index(TP).astype(jnp.int32).reshape(1)
    slots = chips * 4
    shape = jax.ShapeDtypeStruct
    smem = pl.BlockSpec(memory_space=pltpu.SMEM)
    vmem = pl.BlockSpec(memory_space=pltpu.VMEM)
    hbm = pl.BlockSpec(memory_space=pltpu.HBM)

    ids = route_ids.T
    part, new_kv = call(
        attention_kernel,
        [shape((tp_count, rows, LANES), BF), shape((rows, LANES), BF)],
        in_specs=[hbm] * 2 + [smem] + [hbm] * 9,
        scratch=[
            VMEM((span, rows * LANES), BF),
            pltpu.SMEM((rows,), jnp.int32),
            pltpu.SMEM((gates,), F32),
            VMEM((rows, width), BF),
            VMEM((1, width), F32),
            VMEM((2 * hd + gates, width), BF),
            VMEM((2 * hd, width), BF),
            VMEM((hd, width), BF),
            VMEM((rows, 1, span), F32),
            VMEM((span, LANES), F32),
            pltpu.SemaphoreType.DMA((rows,)),
            pltpu.SemaphoreType.DMA((11,)),
        ],
        limit=24 << 20,
    )(
        far(lengths),
        far(forget_bias),
        tp,
        far(layer_in),
        far(attn_gain.reshape(1, width)),
        far(query_weight.T),
        far(key_weight.T),
        far(value_weight.T),
        far(forget_weight.T),
        far(out_weight),
        far(cum_gates),
        far(kv_cache),
    )
    arrived = exchange(part, TP)
    middle, send = call(
        middle_kernel,
        [shape((rows, LANES), BF), shape((slots, LANES), BF)],
        in_specs=[smem] + [vmem] * 3,
    )(tp, arrived, layer_in, ids)
    mine = exchange(send.reshape(chips, 4, LANES), CHIPS).reshape(slots, LANES)
    theirs = lax.ppermute(mine, "c", SWAP)
    keep, give = call(
        expert_kernel,
        [shape((slots, LANES), F32), shape((slots, LANES), BF)],
        in_specs=[smem] + [vmem] * 8 + [hbm],
        scratch=[
            VMEM((slots, LANES), F32),
            VMEM((slots, LANES), F32),
            VMEM(shared_down.shape, BF),
            pltpu.SemaphoreType.DMA,
        ],
    )(
        core,
        mine,
        theirs,
        ffn_gain.reshape(1, width),
        expert_gate,
        expert_up,
        expert_down,
        shared_gate.T,
        shared_up.T,
        far(shared_down),
    )
    send = (keep + lax.ppermute(give, "c", SWAP).astype(F32)).astype(BF)
    arrived = exchange(send.reshape(chips, 4, LANES), CHIPS).reshape(slots, LANES)
    send = call(
        combine_kernel, shape((tp_count, rows, LANES), BF), in_specs=[vmem] * 4
    )(arrived, ids, route_weights.T, middle)
    out = exchange(send, TP)
    layer_out = out.transpose(1, 0, 2).reshape(rows, width)
    return (layer_out, new_kv.reshape(rows, 1, LANES))


def solution(mesh):
    split = Mesh(mesh.devices.reshape(4, 4, 8, 2), ALL)
    placed = (
        P(EP, None),
        P(),
        P(None, TP),
        P(None, TP),
        P(None, TP),
        P(),
        P(),
        P(TP, None),
        P(EP, TP, None, None),
        P(EP, TP, None),
        P(EP),
        P(),
        P(EP, None),
        P(EP, None),
        P(None, TP),
        P(None, TP),
        P(TP, None),
        P(ALL, None, None),
        P(ALL, None, None),
        P(ALL, None, None),
    )
    return jax.shard_map(
        body,
        mesh=split,
        in_specs=placed,
        out_specs=(P(EP, None), P(EP, TP, None)),
        check_vma=False,
    )
```

```python
import functools

import jax
import jax.numpy as jnp
from jax import lax
from jax.experimental import pallas as pl
from jax.experimental.pallas import tpu as pltpu
from jax.sharding import Mesh, PartitionSpec as P

NORM_EPS = 1e-06
BF = jnp.bfloat16
F32 = jnp.float32
LANES = 128
VMEM = pltpu.VMEM
EP = ("y", "x")
TP = ("z", "c")
ALL = ("y", "x", "z", "c")
CHIPS = ("y", "x", "z")
SWAP = ((0, 1), (1, 0))


def nt(a, b):
    return lax.dot_general(a, b, (((1,), (1,)), ((), ())), preferred_element_type=F32)


def tn(a, b):
    return lax.dot_general(a, b, (((0,), (0,)), ((), ())), preferred_element_type=F32)


def mm(a, b):
    return jnp.dot(a, b, preferred_element_type=F32)


def rms_rows(wide, gain):
    factor = lax.rsqrt(jnp.mean(wide * wide, axis=-1, keepdims=True) + NORM_EPS)
    return (wide * factor * gain).astype(BF)


def attention_kernel(
    lengths_hbm,
    bias_hbm,
    head_ref,
    layer_hbm,
    gain_hbm,
    wq_hbm,
    wk_hbm,
    wv_hbm,
    wf_hbm,
    wo_hbm,
    cum_hbm,
    kv_hbm,
    part_ref,
    newkv_ref,
    kv_buf,
    lengths_ref,
    bias_ref,
    layer_ref,
    gain_ref,
    first_ref,
    second_ref,
    wo_ref,
    cum_ref,
    score_ref,
    kv_sems,
    sems,
):
    rows, width = layer_ref.shape
    span = kv_hbm.shape[2]
    hd = wq_hbm.shape[0]
    gates = wf_hbm.shape[0]
    pairs = (
        (layer_hbm, layer_ref),
        (gain_hbm, gain_ref),
        (wq_hbm, first_ref.at[:hd]),
        (wk_hbm, first_ref.at[hd : 2 * hd]),
        (wf_hbm, first_ref.at[2 * hd :]),
        (cum_hbm, cum_ref),
        (wv_hbm, second_ref),
        (wo_hbm, wo_ref),
        (lengths_hbm, lengths_ref),
        (bias_hbm, bias_ref),
    )
    small = [pltpu.make_async_copy(a, b, sems.at[i]) for i, (a, b) in enumerate(pairs)]
    group = 8

    def fetch(s):
        at = pl.multiple_of(s * LANES, LANES)
        return pltpu.make_async_copy(kv_hbm.at[s, 0], kv_buf.at[:, pl.ds(at, LANES)], kv_sems.at[s])

    def start(s, carry):
        fetch(s).start()
        return carry

    for copy in small:
        copy.start()
    lax.fori_loop(0, rows, start, 0)

    for copy in small[:5] + small[8:]:
        copy.wait()
    lane = lax.broadcasted_iota(jnp.int32, (1, LANES), 1)
    length = jnp.zeros((1, LANES), jnp.int32)
    for s in range(rows):
        length = jnp.where(lane == s, lengths_ref[s], length)

    normed = rms_rows(layer_ref[...].astype(F32), gain_ref[...])
    padded = jnp.concatenate([normed, jnp.zeros((LANES - rows, width), BF)], axis=0)
    by_seq = nt(first_ref[...], padded)
    query = by_seq[:hd].astype(BF).astype(F32)
    key = by_seq[hd : 2 * hd].astype(BF).astype(F32)

    scaling = hd ** (-0.5)
    query = query * scaling
    itself = jnp.sum(query * key, axis=0, keepdims=True)
    head = head_ref[0]
    head_row = lax.broadcasted_iota(jnp.int32, (gates, LANES), 0) == head
    logit = (
        jnp.sum(jnp.where(head_row, by_seq[2 * hd :], 0.0), axis=0, keepdims=True) + bias_ref[head]
    )
    forget = -(jnp.maximum(-logit, 0.0) + jnp.log1p(jnp.exp(-jnp.abs(logit))))

    small[5].wait()
    cum = cum_ref[...].reshape(rows, span)
    cum = jnp.concatenate([cum, jnp.zeros((LANES - rows, span), F32)], axis=0)
    cum = jnp.transpose(cum)
    position = lax.broadcasted_iota(jnp.int32, (span, LANES), 0)
    latest = jnp.sum(jnp.where(position == length - 1, cum, 0.0), axis=0, keepdims=True)
    shift = (latest + forget) - cum

    for copy in small[6:8]:
        copy.wait()
    new_kv = nt(normed, jnp.concatenate([first_ref[hd : 2 * hd], second_ref[...]], axis=0))
    new_kv = new_kv.astype(BF)
    newkv_ref[...] = new_kv
    query = jnp.concatenate([query, jnp.zeros((LANES - hd, LANES), F32)], axis=0)
    lane_full = lax.broadcasted_iota(jnp.int32, (LANES, LANES), 1)
    score_ref[...] = shift

    def score_step(j, carry):
        first = j * group
        spread = jnp.concatenate(
            [jnp.where(lane_full == first + k, query, 0.0).astype(BF) for k in range(group)],
            axis=0,
        )
        for k in range(group):
            fetch(first + k).wait()
        at = pl.multiple_of(first * LANES, LANES)
        score_ref[...] += mm(kv_buf[:, pl.ds(at, group * LANES)], spread)
        return carry

    lax.fori_loop(0, rows // group, score_step, 0)
    scores = score_ref[...]
    scores = jnp.where(position < length, scores, -jnp.inf)
    highest = jnp.maximum(jnp.max(scores, axis=0, keepdims=True), itself)
    earlier = jnp.exp(scores - highest)
    own = jnp.exp(itself - highest)
    inverse = 1.0 / (jnp.sum(earlier, axis=0, keepdims=True) + own)
    probs = jnp.transpose(earlier * inverse)[:rows].astype(BF)
    own = (own * inverse).astype(BF).astype(F32)

    square_row = lax.broadcasted_iota(jnp.int32, (rows, LANES), 0)
    square_lane = lax.broadcasted_iota(jnp.int32, (rows, LANES), 1)
    own_column = jnp.sum(
        jnp.where(square_row == square_lane, own, 0.0), axis=1, keepdims=True
    )
    blended = own_column * new_kv.astype(F32)
    step = 16

    def value_step(i, total):
        for k in range(step):
            s = (i * step + k) * 2
            at = pl.multiple_of(s * LANES, LANES)
            two = mm(probs, kv_buf[:, pl.ds(at, 2 * LANES)])
            total = total + jnp.where(square_row == s, two[:, :LANES], 0.0)
            total = total + jnp.where(square_row == s + 1, two[:, LANES:], 0.0)
        return total

    blended = lax.fori_loop(0, rows // (2 * step), value_step, blended)
    attended = blended[:, hd:].astype(BF)
    out = mm(attended, wo_ref[...])
    for t in range(part_ref.shape[0]):
        part_ref[t] = out[:, t * LANES : (t + 1) * LANES].astype(BF)


def routing(ids_ref, weights_ref, many):
    picks, rows = ids_ref.shape
    square = lax.broadcasted_iota(jnp.int32, (rows, rows), 0) == lax.broadcasted_iota(
        jnp.int32, (rows, rows), 1
    )
    slot = lax.broadcasted_iota(jnp.int32, (rows, many), 1)
    row = lax.broadcasted_iota(jnp.int32, (rows, many), 0)
    expert = slot >> 2
    kind = slot & 3
    weight = jnp.zeros((rows, many), F32)
    member = jnp.zeros((rows, many), F32)
    for k in range(picks):
        ids = ids_ref[k : k + 1, :].astype(F32)
        column = jnp.sum(jnp.where(square, ids, 0.0), axis=1, keepdims=True).astype(jnp.int32)
        match = column == expert
        member = jnp.where(match, 1.0, member)
        if weights_ref is not None:
            share = weights_ref[k : k + 1, :]
            share = jnp.sum(jnp.where(square, share, 0.0), axis=1, keepdims=True)
            weight = jnp.where(match, share, weight)
    named = member > 0.0
    lowest = jnp.min(jnp.where(named, row, rows), axis=0, keepdims=True)
    highest = jnp.max(jnp.where(named, row, -1), axis=0, keepdims=True)
    wanted = jnp.where(kind == 0, lowest, jnp.where(highest == lowest, -1, highest))
    routed = jnp.where(row == wanted, member, 0.0)
    own = jnp.where(row == ((slot >> 5) * 2 + kind - 2), 1.0, 0.0)
    if weights_ref is not None:
        routed = routed * weight
    return jnp.where(kind < 2, routed, own)


def middle_kernel(tp_ref, arrived_ref, layer_ref, ids_ref, middle_ref, send_ref):
    place = routing(ids_ref, None, send_ref.shape[0]).astype(BF)
    total = arrived_ref[0].astype(F32)
    for t in range(1, arrived_ref.shape[0]):
        total = total + arrived_ref[t].astype(F32)
    start = pl.multiple_of(tp_ref[0] * LANES, LANES)
    middle = (layer_ref[:, pl.ds(start, LANES)].astype(F32) + total).astype(BF)
    middle_ref[...] = middle
    send_ref[...] = tn(place, middle).astype(BF)


def expert_kernel(
    core_ref,
    mine_ref,
    theirs_ref,
    gain_ref,
    gate_ref,
    up_ref,
    down_ref,
    sgate_ref,
    sup_ref,
    sdown_ref,
    keep_ref,
    give_ref,
    even_ref,
    odd_ref,
):
    groups = 16
    kinds = 4
    stride = mine_ref.shape[0] // groups
    tiles = stride // kinds
    first = core_ref[0] == 0
    mine = mine_ref[...].astype(F32)
    theirs = theirs_ref[...].astype(F32)
    even_ref[...] = jnp.where(first, mine, theirs)
    odd_ref[...] = jnp.where(first, theirs, mine)
    sides = (even_ref, odd_ref)

    def rows_of(s):
        return jnp.concatenate(
            [
                sides[t % 2][pl.ds((t // 2) * kinds + s, groups, stride=stride), :]
                for t in range(2 * tiles)
            ],
            axis=1,
        )

    def swish(v):
        return v / (1.0 + jnp.exp(-v))

    gain = gain_ref[...]
    routed = rms_rows(jnp.concatenate([rows_of(0), rows_of(1)], axis=0), gain)
    shared = rms_rows(jnp.concatenate([rows_of(2), rows_of(3)], axis=0), gain)
    hidden = (swish(mm(routed, gate_ref[0])) * mm(routed, up_ref[0])).astype(BF)
    served = mm(hidden, down_ref[0])
    shidden = (swish(nt(shared, sgate_ref[...])) * nt(shared, sup_ref[...])).astype(BF)
    sserved = mm(shidden, sdown_ref[...])
    for s, block in enumerate((served, served, sserved, sserved)):
        for t in range(2 * tiles):
            sides[t % 2][pl.ds((t // 2) * kinds + s, groups, stride=stride), :] = block[
                (s % 2) * groups : (s % 2 + 1) * groups, t * LANES : (t + 1) * LANES
            ]
    even = even_ref[...]
    odd = odd_ref[...]
    keep_ref[...] = jnp.where(first, even, odd)
    give_ref[...] = jnp.where(first, odd, even).astype(BF)


def combine_kernel(arrived_ref, ids_ref, weights_ref, middle_ref, send_ref):
    shares = routing(ids_ref, weights_ref, arrived_ref.shape[0])
    high = shares.astype(BF)
    low = (shares - high.astype(F32)).astype(BF)
    arrived = arrived_ref[...]
    total = mm(high, arrived) + mm(low, arrived)
    out = (middle_ref[...].astype(F32) + total).astype(BF)
    for t in range(send_ref.shape[0]):
        send_ref[t] = out


def exchange(x, axes):
    return lax.all_to_all(x, axes, split_axis=0, concat_axis=0, tiled=True)


def far(x):
    return pltpu.with_memory_space_constraint(x, pltpu.HBM)


def call(kernel, outs, in_specs, scratch=(), limit=16 << 20):
    return pl.pallas_call(
        kernel,
        out_shape=outs,
        in_specs=in_specs,
        scratch_shapes=list(scratch),
        compiler_params=pltpu.CompilerParams(vmem_limit_bytes=limit),
    )


def body(
    layer_in,
    attn_gain,
    query_weight,
    key_weight,
    value_weight,
    forget_weight,
    forget_bias,
    out_weight,
    kv_cache,
    cum_gates,
    lengths,
    ffn_gain,
    route_ids,
    route_weights,
    shared_gate,
    shared_up,
    shared_down,
    expert_gate,
    expert_up,
    expert_down,
):
    rows, width = layer_in.shape
    span = kv_cache.shape[2]
    hd = query_weight.shape[1]
    gates = forget_weight.shape[1]
    tp_count = lax.axis_size(TP)
    chips = lax.axis_size(CHIPS)
    core = lax.axis_index("c").astype(jnp.int32).reshape(1)
    tp = lax.axis_index(TP).astype(jnp.int32).reshape(1)
    slots = chips * 4
    shape = jax.ShapeDtypeStruct
    smem = pl.BlockSpec(memory_space=pltpu.SMEM)
    vmem = pl.BlockSpec(memory_space=pltpu.VMEM)
    hbm = pl.BlockSpec(memory_space=pltpu.HBM)

    ids = route_ids.T
    part, new_kv = call(
        attention_kernel,
        [shape((tp_count, rows, LANES), BF), shape((rows, LANES), BF)],
        in_specs=[hbm] * 2 + [smem] + [hbm] * 9,
        scratch=[
            VMEM((span, rows * LANES), BF),
            pltpu.SMEM((rows,), jnp.int32),
            pltpu.SMEM((gates,), F32),
            VMEM((rows, width), BF),
            VMEM((1, width), F32),
            VMEM((2 * hd + gates, width), BF),
            VMEM((hd, width), BF),
            VMEM((hd, width), BF),
            VMEM((rows, 1, span), F32),
            VMEM((span, LANES), F32),
            pltpu.SemaphoreType.DMA((rows,)),
            pltpu.SemaphoreType.DMA((10,)),
        ],
        limit=24 << 20,
    )(
        far(lengths),
        far(forget_bias),
        tp,
        far(layer_in),
        far(attn_gain.reshape(1, width)),
        far(query_weight.T),
        far(key_weight.T),
        far(value_weight.T),
        far(forget_weight.T),
        far(out_weight),
        far(cum_gates),
        far(kv_cache),
    )
    arrived = exchange(part, TP)
    middle, send = call(
        middle_kernel,
        [shape((rows, LANES), BF), shape((slots, LANES), BF)],
        in_specs=[smem] + [vmem] * 3,
    )(tp, arrived, layer_in, ids)
    mine = exchange(send.reshape(chips, 4, LANES), CHIPS).reshape(slots, LANES)
    theirs = lax.ppermute(mine, "c", SWAP)
    keep, give = call(
        expert_kernel,
        [shape((slots, LANES), F32), shape((slots, LANES), BF)],
        in_specs=[smem] + [vmem] * 9,
        scratch=[VMEM((slots, LANES), F32)] * 2,
    )(
        core,
        mine,
        theirs,
        ffn_gain.reshape(1, width),
        expert_gate,
        expert_up,
        expert_down,
        shared_gate.T,
        shared_up.T,
        shared_down,
    )
    send = (keep + lax.ppermute(give, "c", SWAP).astype(F32)).astype(BF)
    arrived = exchange(send.reshape(chips, 4, LANES), CHIPS).reshape(slots, LANES)
    send = call(
        combine_kernel, shape((tp_count, rows, LANES), BF), in_specs=[vmem] * 4
    )(arrived, ids, route_weights.T, middle)
    out = exchange(send, TP)
    layer_out = out.transpose(1, 0, 2).reshape(rows, width)
    return (layer_out, new_kv.reshape(rows, 1, LANES))


def solution(mesh):
    split = Mesh(mesh.devices.reshape(4, 4, 8, 2), ALL)
    placed = (
        P(EP, None),
        P(),
        P(None, TP),
        P(None, TP),
        P(None, TP),
        P(),
        P(),
        P(TP, None),
        P(EP, TP, None, None),
        P(EP, TP, None),
        P(EP),
        P(),
        P(EP, None),
        P(EP, None),
        P(None, TP),
        P(None, TP),
        P(TP, None),
        P(ALL, None, None),
        P(ALL, None, None),
        P(ALL, None, None),
    )
    return jax.shard_map(
        body,
        mesh=split,
        in_specs=placed,
        out_specs=(P(EP, None), P(EP, TP, None)),
        check_vma=False,
    )
```

```python
import functools

import jax
import jax.numpy as jnp
from jax import lax
from jax.experimental import pallas as pl
from jax.experimental.pallas import tpu as pltpu
from jax.sharding import Mesh, PartitionSpec as P

NORM_EPS = 1e-06
BF = jnp.bfloat16
F32 = jnp.float32
LANES = 128
VMEM = pltpu.VMEM
EP = ("y", "x")
TP = ("z", "c")
ALL = ("y", "x", "z", "c")
CHIPS = ("y", "x", "z")
SWAP = ((0, 1), (1, 0))


def nt(a, b):
    return lax.dot_general(a, b, (((1,), (1,)), ((), ())), preferred_element_type=F32)


def tn(a, b):
    return lax.dot_general(a, b, (((0,), (0,)), ((), ())), preferred_element_type=F32)


def mm(a, b):
    return jnp.dot(a, b, preferred_element_type=F32)


def rms_rows(wide, gain):
    factor = lax.rsqrt(jnp.mean(wide * wide, axis=-1, keepdims=True) + NORM_EPS)
    return (wide * factor * gain).astype(BF)


def attention_kernel(
    lengths_hbm,
    bias_hbm,
    head_ref,
    layer_hbm,
    gain_hbm,
    wq_hbm,
    wk_hbm,
    wv_hbm,
    wf_hbm,
    wo_hbm,
    cum_hbm,
    kv_hbm,
    part_ref,
    newkv_ref,
    kv_buf,
    lengths_ref,
    bias_ref,
    layer_ref,
    gain_ref,
    first_ref,
    wo_ref,
    cum_ref,
    score_ref,
    kv_sems,
    sems,
):
    rows, width = layer_ref.shape
    span = kv_hbm.shape[2]
    hd = wq_hbm.shape[0]
    gates = wf_hbm.shape[0]
    pairs = (
        (layer_hbm, layer_ref),
        (gain_hbm, gain_ref),
        (wq_hbm, first_ref.at[:hd]),
        (wk_hbm, first_ref.at[hd : 2 * hd]),
        (wv_hbm, first_ref.at[2 * hd : 3 * hd]),
        (wf_hbm, first_ref.at[3 * hd :]),
        (cum_hbm, cum_ref),
        (wo_hbm, wo_ref),
        (lengths_hbm, lengths_ref),
        (bias_hbm, bias_ref),
    )
    small = [pltpu.make_async_copy(a, b, sems.at[i]) for i, (a, b) in enumerate(pairs)]
    group = 8

    def fetch(s):
        at = pl.multiple_of(s * LANES, LANES)
        return pltpu.make_async_copy(kv_hbm.at[s, 0], kv_buf.at[:, pl.ds(at, LANES)], kv_sems.at[s])

    def start(s, carry):
        fetch(s).start()
        return carry

    for copy in small:
        copy.start()
    lax.fori_loop(0, rows, start, 0)

    for copy in small[:6] + small[8:]:
        copy.wait()
    lane = lax.broadcasted_iota(jnp.int32, (1, LANES), 1)
    length = jnp.zeros((1, LANES), jnp.int32)
    for s in range(rows):
        length = jnp.where(lane == s, lengths_ref[s], length)

    normed = rms_rows(layer_ref[...].astype(F32), gain_ref[...])
    padded = jnp.concatenate([normed, jnp.zeros((LANES - rows, width), BF)], axis=0)
    by_seq = nt(first_ref[...], padded)
    query = by_seq[:hd].astype(BF).astype(F32)
    key = by_seq[hd : 2 * hd].astype(BF).astype(F32)

    scaling = hd ** (-0.5)
    query = query * scaling
    itself = jnp.sum(query * key, axis=0, keepdims=True)
    head = head_ref[0]
    head_row = lax.broadcasted_iota(jnp.int32, (gates, LANES), 0) == head
    logit = (
        jnp.sum(jnp.where(head_row, by_seq[3 * hd :], 0.0), axis=0, keepdims=True) + bias_ref[head]
    )
    forget = -(jnp.maximum(-logit, 0.0) + jnp.log1p(jnp.exp(-jnp.abs(logit))))

    small[6].wait()
    cum = cum_ref[...].reshape(rows, span)
    cum = jnp.concatenate([cum, jnp.zeros((LANES - rows, span), F32)], axis=0)
    cum = jnp.transpose(cum)
    position = lax.broadcasted_iota(jnp.int32, (span, LANES), 0)
    latest = jnp.sum(jnp.where(position == length - 1, cum, 0.0), axis=0, keepdims=True)
    shift = (latest + forget) - cum

    new_kv = jnp.transpose(by_seq[hd : 3 * hd])[:rows].astype(BF)
    newkv_ref[...] = new_kv
    query = jnp.concatenate([query, jnp.zeros((LANES - hd, LANES), F32)], axis=0)
    lane_full = lax.broadcasted_iota(jnp.int32, (LANES, LANES), 1)
    score_ref[...] = shift

    def score_step(j, carry):
        first = j * group
        spread = jnp.concatenate(
            [jnp.where(lane_full == first + k, query, 0.0).astype(BF) for k in range(group)],
            axis=0,
        )
        for k in range(group):
            fetch(first + k).wait()
        at = pl.multiple_of(first * LANES, LANES)
        score_ref[...] += mm(kv_buf[:, pl.ds(at, group * LANES)], spread)
        return carry

    lax.fori_loop(0, rows // group, score_step, 0)
    scores = score_ref[...]
    scores = jnp.where(position < length, scores, -jnp.inf)
    highest = jnp.maximum(jnp.max(scores, axis=0, keepdims=True), itself)
    earlier = jnp.exp(scores - highest)
    own = jnp.exp(itself - highest)
    inverse = 1.0 / (jnp.sum(earlier, axis=0, keepdims=True) + own)
    probs = jnp.transpose(earlier * inverse)[:rows].astype(BF)
    own = (own * inverse).astype(BF).astype(F32)

    square_row = lax.broadcasted_iota(jnp.int32, (rows, LANES), 0)
    square_lane = lax.broadcasted_iota(jnp.int32, (rows, LANES), 1)
    own_column = jnp.sum(
        jnp.where(square_row == square_lane, own, 0.0), axis=1, keepdims=True
    )
    blended = own_column * new_kv.astype(F32)
    half = rows // 2
    parts = []
    for h in range(0, rows, half):
        some = probs[h : h + half]
        mark = lax.broadcasted_iota(jnp.int32, (half, LANES), 0) + h
        total = blended[h : h + half]
        for s in range(h, h + half, 2):
            two = mm(some, kv_buf[:, s * LANES : (s + 2) * LANES])
            total = total + jnp.where(mark == s, two[:, :LANES], 0.0)
            total = total + jnp.where(mark == s + 1, two[:, LANES:], 0.0)
        parts.append(total)
    blended = jnp.concatenate(parts, axis=0)
    attended = blended[:, hd:].astype(BF)
    small[7].wait()
    out = mm(attended, wo_ref[...])
    for t in range(part_ref.shape[0]):
        part_ref[t] = out[:, t * LANES : (t + 1) * LANES].astype(BF)


def routing(ids_ref, weights_ref, many):
    picks, rows = ids_ref.shape
    square = lax.broadcasted_iota(jnp.int32, (rows, rows), 0) == lax.broadcasted_iota(
        jnp.int32, (rows, rows), 1
    )
    slot = lax.broadcasted_iota(jnp.int32, (rows, many), 1)
    row = lax.broadcasted_iota(jnp.int32, (rows, many), 0)
    expert = slot >> 2
    kind = slot & 3
    weight = jnp.zeros((rows, many), F32)
    member = jnp.zeros((rows, many), F32)
    for k in range(picks):
        ids = ids_ref[k : k + 1, :].astype(F32)
        column = jnp.sum(jnp.where(square, ids, 0.0), axis=1, keepdims=True).astype(jnp.int32)
        match = column == expert
        member = jnp.where(match, 1.0, member)
        if weights_ref is not None:
            share = weights_ref[k : k + 1, :]
            share = jnp.sum(jnp.where(square, share, 0.0), axis=1, keepdims=True)
            weight = jnp.where(match, share, weight)
    named = member > 0.0
    lowest = jnp.min(jnp.where(named, row, rows), axis=0, keepdims=True)
    highest = jnp.max(jnp.where(named, row, -1), axis=0, keepdims=True)
    wanted = jnp.where(kind == 0, lowest, jnp.where(highest == lowest, -1, highest))
    routed = jnp.where(row == wanted, member, 0.0)
    own = jnp.where(row == ((slot >> 5) * 2 + kind - 2), 1.0, 0.0)
    if weights_ref is not None:
        routed = routed * weight
    return jnp.where(kind < 2, routed, own)


def middle_kernel(tp_ref, arrived_ref, layer_ref, ids_ref, middle_ref, send_ref):
    place = routing(ids_ref, None, send_ref.shape[0]).astype(BF)
    total = arrived_ref[0].astype(F32)
    for t in range(1, arrived_ref.shape[0]):
        total = total + arrived_ref[t].astype(F32)
    start = pl.multiple_of(tp_ref[0] * LANES, LANES)
    middle = (layer_ref[:, pl.ds(start, LANES)].astype(F32) + total).astype(BF)
    middle_ref[...] = middle
    send_ref[...] = tn(place, middle).astype(BF)


def expert_kernel(
    core_ref,
    mine_ref,
    theirs_ref,
    gain_ref,
    gate_ref,
    up_ref,
    down_ref,
    sgate_ref,
    sup_ref,
    sdown_ref,
    keep_ref,
    give_ref,
    even_ref,
    odd_ref,
):
    groups = 16
    kinds = 4
    stride = mine_ref.shape[0] // groups
    tiles = stride // kinds
    first = core_ref[0] == 0
    mine = mine_ref[...].astype(F32)
    theirs = theirs_ref[...].astype(F32)
    even_ref[...] = jnp.where(first, mine, theirs)
    odd_ref[...] = jnp.where(first, theirs, mine)
    sides = (even_ref, odd_ref)

    def rows_of(s):
        return jnp.concatenate(
            [
                sides[t % 2][pl.ds((t // 2) * kinds + s, groups, stride=stride), :]
                for t in range(2 * tiles)
            ],
            axis=1,
        )

    def swish(v):
        return v / (1.0 + jnp.exp(-v))

    gain = gain_ref[...]
    routed = rms_rows(jnp.concatenate([rows_of(0), rows_of(1)], axis=0), gain)
    shared = rms_rows(jnp.concatenate([rows_of(2), rows_of(3)], axis=0), gain)
    hidden = (swish(mm(routed, gate_ref[0])) * mm(routed, up_ref[0])).astype(BF)
    served = mm(hidden, down_ref[0])
    shidden = (swish(nt(shared, sgate_ref[...])) * nt(shared, sup_ref[...])).astype(BF)
    sserved = mm(shidden, sdown_ref[...])
    for s, block in enumerate((served, served, sserved, sserved)):
        for t in range(2 * tiles):
            sides[t % 2][pl.ds((t // 2) * kinds + s, groups, stride=stride), :] = block[
                (s % 2) * groups : (s % 2 + 1) * groups, t * LANES : (t + 1) * LANES
            ]
    even = even_ref[...]
    odd = odd_ref[...]
    keep_ref[...] = jnp.where(first, even, odd)
    give_ref[...] = jnp.where(first, odd, even).astype(BF)


def combine_kernel(arrived_ref, ids_ref, weights_ref, middle_ref, send_ref):
    shares = routing(ids_ref, weights_ref, arrived_ref.shape[0])
    high = shares.astype(BF)
    low = (shares - high.astype(F32)).astype(BF)
    arrived = arrived_ref[...]
    total = mm(high, arrived) + mm(low, arrived)
    out = (middle_ref[...].astype(F32) + total).astype(BF)
    for t in range(send_ref.shape[0]):
        send_ref[t] = out


def exchange(x, axes):
    return lax.all_to_all(x, axes, split_axis=0, concat_axis=0, tiled=True)


def far(x):
    return pltpu.with_memory_space_constraint(x, pltpu.HBM)


def call(kernel, outs, in_specs, scratch=(), limit=16 << 20):
    return pl.pallas_call(
        kernel,
        out_shape=outs,
        in_specs=in_specs,
        scratch_shapes=list(scratch),
        compiler_params=pltpu.CompilerParams(vmem_limit_bytes=limit),
    )


def body(
    layer_in,
    attn_gain,
    query_weight,
    key_weight,
    value_weight,
    forget_weight,
    forget_bias,
    out_weight,
    kv_cache,
    cum_gates,
    lengths,
    ffn_gain,
    route_ids,
    route_weights,
    shared_gate,
    shared_up,
    shared_down,
    expert_gate,
    expert_up,
    expert_down,
):
    rows, width = layer_in.shape
    span = kv_cache.shape[2]
    hd = query_weight.shape[1]
    gates = forget_weight.shape[1]
    tp_count = lax.axis_size(TP)
    chips = lax.axis_size(CHIPS)
    core = lax.axis_index("c").astype(jnp.int32).reshape(1)
    tp = lax.axis_index(TP).astype(jnp.int32).reshape(1)
    slots = chips * 4
    shape = jax.ShapeDtypeStruct
    smem = pl.BlockSpec(memory_space=pltpu.SMEM)
    vmem = pl.BlockSpec(memory_space=pltpu.VMEM)
    hbm = pl.BlockSpec(memory_space=pltpu.HBM)

    ids = route_ids.T
    part, new_kv = call(
        attention_kernel,
        [shape((tp_count, rows, LANES), BF), shape((rows, LANES), BF)],
        in_specs=[hbm] * 2 + [smem] + [hbm] * 9,
        scratch=[
            VMEM((span, rows * LANES), BF),
            pltpu.SMEM((rows,), jnp.int32),
            pltpu.SMEM((gates,), F32),
            VMEM((rows, width), BF),
            VMEM((1, width), F32),
            VMEM((3 * hd + gates, width), BF),
            VMEM((hd, width), BF),
            VMEM((rows, 1, span), F32),
            VMEM((span, LANES), F32),
            pltpu.SemaphoreType.DMA((rows,)),
            pltpu.SemaphoreType.DMA((10,)),
        ],
        limit=24 << 20,
    )(
        far(lengths),
        far(forget_bias),
        tp,
        far(layer_in),
        far(attn_gain.reshape(1, width)),
        far(query_weight.T),
        far(key_weight.T),
        far(value_weight.T),
        far(forget_weight.T),
        far(out_weight),
        far(cum_gates),
        far(kv_cache),
    )
    arrived = exchange(part, TP)
    middle, send = call(
        middle_kernel,
        [shape((rows, LANES), BF), shape((slots, LANES), BF)],
        in_specs=[smem] + [vmem] * 3,
    )(tp, arrived, layer_in, ids)
    mine = exchange(send.reshape(chips, 4, LANES), CHIPS).reshape(slots, LANES)
    theirs = lax.ppermute(mine, "c", SWAP)
    keep, give = call(
        expert_kernel,
        [shape((slots, LANES), F32), shape((slots, LANES), BF)],
        in_specs=[smem] + [vmem] * 9,
        scratch=[VMEM((slots, LANES), F32)] * 2,
    )(
        core,
        mine,
        theirs,
        ffn_gain.reshape(1, width),
        expert_gate,
        expert_up,
        expert_down,
        shared_gate.T,
        shared_up.T,
        shared_down,
    )
    send = (keep + lax.ppermute(give, "c", SWAP).astype(F32)).astype(BF)
    arrived = exchange(send.reshape(chips, 4, LANES), CHIPS).reshape(slots, LANES)
    send = call(
        combine_kernel, shape((tp_count, rows, LANES), BF), in_specs=[vmem] * 4
    )(arrived, ids, route_weights.T, middle)
    out = exchange(send, TP)
    layer_out = out.transpose(1, 0, 2).reshape(rows, width)
    return (layer_out, new_kv.reshape(rows, 1, LANES))


def solution(mesh):
    split = Mesh(mesh.devices.reshape(4, 4, 8, 2), ALL)
    placed = (
        P(EP, None),
        P(),
        P(None, TP),
        P(None, TP),
        P(None, TP),
        P(),
        P(),
        P(TP, None),
        P(EP, TP, None, None),
        P(EP, TP, None),
        P(EP),
        P(),
        P(EP, None),
        P(EP, None),
        P(None, TP),
        P(None, TP),
        P(TP, None),
        P(ALL, None, None),
        P(ALL, None, None),
        P(ALL, None, None),
    )
    return jax.shard_map(
        body,
        mesh=split,
        in_specs=placed,
        out_specs=(P(EP, None), P(EP, TP, None)),
        check_vma=False,
    )
```

```python
import functools

import jax
import jax.numpy as jnp
from jax import lax
from jax.experimental import pallas as pl
from jax.experimental.pallas import tpu as pltpu
from jax.sharding import Mesh, PartitionSpec as P

NORM_EPS = 1e-06
BF = jnp.bfloat16
F32 = jnp.float32
LANES = 128
VMEM = pltpu.VMEM
EP = ("y", "x")
TP = ("z", "c")
ALL = ("y", "x", "z", "c")
CHIPS = ("y", "x", "z")
SWAP = ((0, 1), (1, 0))


def nt(a, b):
    return lax.dot_general(a, b, (((1,), (1,)), ((), ())), preferred_element_type=F32)


def tn(a, b):
    return lax.dot_general(a, b, (((0,), (0,)), ((), ())), preferred_element_type=F32)


def mm(a, b):
    return jnp.dot(a, b, preferred_element_type=F32)


def rms_rows(wide, gain):
    factor = lax.rsqrt(jnp.mean(wide * wide, axis=-1, keepdims=True) + NORM_EPS)
    return (wide * factor * gain).astype(BF)


def attention_kernel(
    lengths_hbm,
    bias_hbm,
    head_ref,
    layer_hbm,
    gain_hbm,
    wq_hbm,
    wk_hbm,
    wv_hbm,
    wf_hbm,
    wo_hbm,
    cum_hbm,
    kv_hbm,
    part_ref,
    newkv_ref,
    kv_buf,
    lengths_ref,
    bias_ref,
    layer_ref,
    gain_ref,
    first_ref,
    wo_ref,
    cum_ref,
    score_ref,
    kv_sems,
    sems,
):
    rows, width = layer_ref.shape
    span = kv_hbm.shape[2]
    hd = wq_hbm.shape[0]
    gates = wf_hbm.shape[0]
    pairs = (
        (layer_hbm, layer_ref),
        (gain_hbm, gain_ref),
        (wq_hbm, first_ref.at[:hd]),
        (wk_hbm, first_ref.at[hd : 2 * hd]),
        (wv_hbm, first_ref.at[2 * hd : 3 * hd]),
        (wf_hbm, first_ref.at[3 * hd :]),
        (cum_hbm, cum_ref),
        (wo_hbm, wo_ref),
        (lengths_hbm, lengths_ref),
        (bias_hbm, bias_ref),
    )
    small = [pltpu.make_async_copy(a, b, sems.at[i]) for i, (a, b) in enumerate(pairs)]
    group = 8

    def fetch(s):
        at = pl.multiple_of(s * LANES, LANES)
        return pltpu.make_async_copy(kv_hbm.at[s, 0], kv_buf.at[:, pl.ds(at, LANES)], kv_sems.at[s])

    def start(s, carry):
        fetch(s).start()
        return carry

    for copy in small:
        copy.start()
    lax.fori_loop(0, rows, start, 0)

    for copy in small[:6] + small[8:]:
        copy.wait()
    lane = lax.broadcasted_iota(jnp.int32, (1, LANES), 1)
    length = jnp.zeros((1, LANES), jnp.int32)
    for s in range(rows):
        length = jnp.where(lane == s, lengths_ref[s], length)

    normed = rms_rows(layer_ref[...].astype(F32), gain_ref[...])
    padded = jnp.concatenate([normed, jnp.zeros((LANES - rows, width), BF)], axis=0)
    by_seq = nt(first_ref[...], padded)
    query = by_seq[:hd].astype(BF).astype(F32)
    key = by_seq[hd : 2 * hd].astype(BF).astype(F32)

    scaling = hd ** (-0.5)
    query = query * scaling
    itself = jnp.sum(query * key, axis=0, keepdims=True)
    head = head_ref[0]
    head_row = lax.broadcasted_iota(jnp.int32, (gates, LANES), 0) == head
    logit = (
        jnp.sum(jnp.where(head_row, by_seq[3 * hd :], 0.0), axis=0, keepdims=True) + bias_ref[head]
    )
    forget = -(jnp.maximum(-logit, 0.0) + jnp.log1p(jnp.exp(-jnp.abs(logit))))

    small[6].wait()
    cum = cum_ref[...].reshape(rows, span)
    cum = jnp.concatenate([cum, jnp.zeros((LANES - rows, span), F32)], axis=0)
    cum = jnp.transpose(cum)
    position = lax.broadcasted_iota(jnp.int32, (span, LANES), 0)
    latest = jnp.sum(jnp.where(position == length - 1, cum, 0.0), axis=0, keepdims=True)
    shift = (latest + forget) - cum

    new_kv = jnp.transpose(by_seq[hd : 3 * hd])[:rows].astype(BF)
    newkv_ref[...] = new_kv
    query = jnp.concatenate([query, jnp.zeros((LANES - hd, LANES), F32)], axis=0)
    lane_full = lax.broadcasted_iota(jnp.int32, (LANES, LANES), 1)
    score_ref[...] = shift

    def score_step(j, carry):
        first = j * group
        spread = jnp.concatenate(
            [jnp.where(lane_full == first + k, query, 0.0).astype(BF) for k in range(group)],
            axis=0,
        )
        for k in range(group):
            fetch(first + k).wait()
        at = pl.multiple_of(first * LANES, LANES)
        score_ref[...] += mm(kv_buf[:, pl.ds(at, group * LANES)], spread)
        return carry

    lax.fori_loop(0, rows // group, score_step, 0)
    scores = score_ref[...]
    scores = jnp.where(position < length, scores, -jnp.inf)
    highest = jnp.maximum(jnp.max(scores, axis=0, keepdims=True), itself)
    earlier = jnp.exp(scores - highest)
    own = jnp.exp(itself - highest)
    inverse = 1.0 / (jnp.sum(earlier, axis=0, keepdims=True) + own)
    probs = jnp.transpose(earlier * inverse)[:rows].astype(BF)
    own = (own * inverse).astype(BF).astype(F32)

    square_row = lax.broadcasted_iota(jnp.int32, (rows, LANES), 0)
    square_lane = lax.broadcasted_iota(jnp.int32, (rows, LANES), 1)
    own_column = jnp.sum(
        jnp.where(square_row == square_lane, own, 0.0), axis=1, keepdims=True
    )
    blended = own_column * new_kv.astype(F32)
    half = rows // 2
    parts = []
    for h in range(0, rows, half):
        some = probs[h : h + half]
        mark = lax.broadcasted_iota(jnp.int32, (half, LANES), 0) + h
        total = blended[h : h + half]
        for s in range(h, h + half, 2):
            two = mm(some, kv_buf[:, s * LANES : (s + 2) * LANES])
            total = total + jnp.where(mark == s, two[:, :LANES], 0.0)
            total = total + jnp.where(mark == s + 1, two[:, LANES:], 0.0)
        parts.append(total)
    blended = jnp.concatenate(parts, axis=0)
    attended = blended[:, hd:].astype(BF)
    small[7].wait()
    out = mm(attended, wo_ref[...])
    for t in range(part_ref.shape[0]):
        part_ref[t] = out[:, t * LANES : (t + 1) * LANES].astype(BF)


def routing(ids_ref, weights_ref, many):
    picks, rows = ids_ref.shape
    square = lax.broadcasted_iota(jnp.int32, (rows, rows), 0) == lax.broadcasted_iota(
        jnp.int32, (rows, rows), 1
    )
    slot = lax.broadcasted_iota(jnp.int32, (rows, many), 1)
    row = lax.broadcasted_iota(jnp.int32, (rows, many), 0)
    expert = slot >> 2
    kind = slot & 3
    weight = jnp.zeros((rows, many), F32)
    member = jnp.zeros((rows, many), F32)
    for k in range(picks):
        ids = ids_ref[k : k + 1, :].astype(F32)
        column = jnp.sum(jnp.where(square, ids, 0.0), axis=1, keepdims=True).astype(jnp.int32)
        match = column == expert
        member = jnp.where(match, 1.0, member)
        if weights_ref is not None:
            share = weights_ref[k : k + 1, :]
            share = jnp.sum(jnp.where(square, share, 0.0), axis=1, keepdims=True)
            weight = jnp.where(match, share, weight)
    named = member > 0.0
    lowest = jnp.min(jnp.where(named, row, rows), axis=0, keepdims=True)
    highest = jnp.max(jnp.where(named, row, -1), axis=0, keepdims=True)
    wanted = jnp.where(kind == 0, lowest, jnp.where(highest == lowest, -1, highest))
    routed = jnp.where(row == wanted, member, 0.0)
    own = jnp.where(row == ((slot >> 5) * 2 + kind - 2), 1.0, 0.0)
    if weights_ref is not None:
        routed = routed * weight
    return jnp.where(kind < 2, routed, own)


def middle_kernel(tp_ref, arrived_ref, layer_ref, ids_ref, middle_ref, send_ref):
    place = routing(ids_ref, None, send_ref.shape[0]).astype(BF)
    total = arrived_ref[0].astype(F32)
    for t in range(1, arrived_ref.shape[0]):
        total = total + arrived_ref[t].astype(F32)
    start = pl.multiple_of(tp_ref[0] * LANES, LANES)
    middle = (layer_ref[:, pl.ds(start, LANES)].astype(F32) + total).astype(BF)
    middle_ref[...] = middle
    send_ref[...] = tn(place, middle).astype(BF)


GROUPS = 16
KINDS = 4


def side_products(side, arrived, wide_ref, gain_ref, gate_ref, up_ref, sgate_ref, sup_ref):
    stride = arrived.shape[0] // GROUPS
    tiles = stride // KINDS
    wide_ref[...] = arrived.astype(F32)
    rows = jnp.concatenate(
        [
            jnp.concatenate(
                [wide_ref[pl.ds(t * KINDS + s, GROUPS, stride=stride), :] for t in range(tiles)],
                axis=1,
            )
            for s in range(KINDS)
        ],
        axis=0,
    )
    spans = [
        pl.ds(pl.multiple_of((2 * t + side) * LANES, LANES), LANES) for t in range(tiles)
    ]
    gain = jnp.concatenate([gain_ref[:, at] for at in spans], axis=1)
    squares = jnp.sum(rows * rows, axis=1, keepdims=True)
    scaled = (rows * gain).astype(BF)
    half = scaled.shape[0] // 2
    routed, shared = scaled[:half], scaled[half:]
    return (
        squares,
        mm(routed, jnp.concatenate([gate_ref[0, at, :] for at in spans], axis=0)),
        mm(routed, jnp.concatenate([up_ref[0, at, :] for at in spans], axis=0)),
        nt(shared, jnp.concatenate([sgate_ref[:, at] for at in spans], axis=1)),
        nt(shared, jnp.concatenate([sup_ref[:, at] for at in spans], axis=1)),
    )


def own_kernel(core_ref, mine_ref, *refs):
    weights, (squares_ref, *outs), wide_ref = refs[:5], refs[5:10], refs[10]
    squares, *products = side_products(core_ref[0], mine_ref[...], wide_ref, *weights)
    squares_ref[...] = jnp.broadcast_to(squares, squares_ref.shape)
    for ref, product in zip(outs, products):
        ref[...] = product


def expert_kernel(
    core_ref,
    theirs_ref,
    squares_ref,
    g_ref,
    u_ref,
    sg_ref,
    su_ref,
    gain_ref,
    gate_ref,
    up_ref,
    sgate_ref,
    sup_ref,
    down_ref,
    sdown_ref,
    keep_ref,
    give_ref,
    even_ref,
    odd_ref,
):
    first = core_ref[0] == 0
    squares, g, u, sg, su = side_products(
        1 - core_ref[0],
        theirs_ref[...],
        even_ref,
        gain_ref,
        gate_ref,
        up_ref,
        sgate_ref,
        sup_ref,
    )
    width = gain_ref.shape[1]
    squares = squares + squares_ref[:, :1]
    factor = lax.rsqrt(squares / width + NORM_EPS)
    half = factor.shape[0] // 2

    def swish(v):
        return v / (1.0 + jnp.exp(-v))

    fr, fs = factor[:half], factor[half:]
    hidden = (swish((g + g_ref[...]) * fr) * ((u + u_ref[...]) * fr)).astype(BF)
    served = mm(hidden, down_ref[0])
    shidden = (swish((sg + sg_ref[...]) * fs) * ((su + su_ref[...]) * fs)).astype(BF)
    sserved = mm(shidden, sdown_ref[...])
    sides = (even_ref, odd_ref)
    stride = theirs_ref.shape[0] // GROUPS
    for s, block in enumerate((served, served, sserved, sserved)):
        for t in range(width // LANES):
            sides[t % 2][pl.ds((t // 2) * KINDS + s, GROUPS, stride=stride), :] = block[
                (s % 2) * GROUPS : (s % 2 + 1) * GROUPS, t * LANES : (t + 1) * LANES
            ]
    even = even_ref[...]
    odd = odd_ref[...]
    keep_ref[...] = jnp.where(first, even, odd)
    give_ref[...] = jnp.where(first, odd, even).astype(BF)


def combine_kernel(arrived_ref, ids_ref, weights_ref, middle_ref, send_ref):
    shares = routing(ids_ref, weights_ref, arrived_ref.shape[0])
    high = shares.astype(BF)
    low = (shares - high.astype(F32)).astype(BF)
    arrived = arrived_ref[...]
    total = mm(high, arrived) + mm(low, arrived)
    out = (middle_ref[...].astype(F32) + total).astype(BF)
    for t in range(send_ref.shape[0]):
        send_ref[t] = out


def exchange(x, axes):
    return lax.all_to_all(x, axes, split_axis=0, concat_axis=0, tiled=True)


def far(x):
    return pltpu.with_memory_space_constraint(x, pltpu.HBM)


def call(kernel, outs, in_specs, scratch=(), limit=16 << 20):
    return pl.pallas_call(
        kernel,
        out_shape=outs,
        in_specs=in_specs,
        scratch_shapes=list(scratch),
        compiler_params=pltpu.CompilerParams(vmem_limit_bytes=limit),
    )


def body(
    layer_in,
    attn_gain,
    query_weight,
    key_weight,
    value_weight,
    forget_weight,
    forget_bias,
    out_weight,
    kv_cache,
    cum_gates,
    lengths,
    ffn_gain,
    route_ids,
    route_weights,
    shared_gate,
    shared_up,
    shared_down,
    expert_gate,
    expert_up,
    expert_down,
):
    rows, width = layer_in.shape
    span = kv_cache.shape[2]
    hd = query_weight.shape[1]
    gates = forget_weight.shape[1]
    tp_count = lax.axis_size(TP)
    chips = lax.axis_size(CHIPS)
    core = lax.axis_index("c").astype(jnp.int32).reshape(1)
    tp = lax.axis_index(TP).astype(jnp.int32).reshape(1)
    slots = chips * 4
    shape = jax.ShapeDtypeStruct
    smem = pl.BlockSpec(memory_space=pltpu.SMEM)
    vmem = pl.BlockSpec(memory_space=pltpu.VMEM)
    hbm = pl.BlockSpec(memory_space=pltpu.HBM)

    ids = route_ids.T
    part, new_kv = call(
        attention_kernel,
        [shape((tp_count, rows, LANES), BF), shape((rows, LANES), BF)],
        in_specs=[hbm] * 2 + [smem] + [hbm] * 9,
        scratch=[
            VMEM((span, rows * LANES), BF),
            pltpu.SMEM((rows,), jnp.int32),
            pltpu.SMEM((gates,), F32),
            VMEM((rows, width), BF),
            VMEM((1, width), F32),
            VMEM((3 * hd + gates, width), BF),
            VMEM((hd, width), BF),
            VMEM((rows, 1, span), F32),
            VMEM((span, LANES), F32),
            pltpu.SemaphoreType.DMA((rows,)),
            pltpu.SemaphoreType.DMA((10,)),
        ],
        limit=24 << 20,
    )(
        far(lengths),
        far(forget_bias),
        tp,
        far(layer_in),
        far(attn_gain.reshape(1, width)),
        far(query_weight.T),
        far(key_weight.T),
        far(value_weight.T),
        far(forget_weight.T),
        far(out_weight),
        far(cum_gates),
        far(kv_cache),
    )
    arrived = exchange(part, TP)
    middle, send = call(
        middle_kernel,
        [shape((rows, LANES), BF), shape((slots, LANES), BF)],
        in_specs=[smem] + [vmem] * 3,
    )(tp, arrived, layer_in, ids)
    mine = exchange(send.reshape(chips, 4, LANES), CHIPS).reshape(slots, LANES)
    theirs = lax.ppermute(mine, "c", SWAP)
    sff = shared_gate.shape[1]
    eff = expert_gate.shape[2]
    weights = (
        ffn_gain.reshape(1, width),
        expert_gate,
        expert_up,
        shared_gate.T,
        shared_up.T,
    )
    wide = VMEM((slots, LANES), F32)
    own = call(
        own_kernel,
        [shape((2 * rows, LANES), F32)]
        + [shape((rows, eff), F32)] * 2
        + [shape((rows, sff), F32)] * 2,
        in_specs=[smem] + [vmem] * 6,
        scratch=[wide],
    )(core, mine, *weights)
    keep, give = call(
        expert_kernel,
        [shape((slots, LANES), F32), shape((slots, LANES), BF)],
        in_specs=[smem] + [vmem] * 13,
        scratch=[wide, wide],
    )(core, theirs, *own, *weights, expert_down, shared_down)
    send = (keep + lax.ppermute(give, "c", SWAP).astype(F32)).astype(BF)
    arrived = exchange(send.reshape(chips, 4, LANES), CHIPS).reshape(slots, LANES)
    send = call(
        combine_kernel, shape((tp_count, rows, LANES), BF), in_specs=[vmem] * 4
    )(arrived, ids, route_weights.T, middle)
    out = exchange(send, TP)
    layer_out = out.transpose(1, 0, 2).reshape(rows, width)
    return (layer_out, new_kv.reshape(rows, 1, LANES))


def solution(mesh):
    split = Mesh(mesh.devices.reshape(4, 4, 8, 2), ALL)
    placed = (
        P(EP, None),
        P(),
        P(None, TP),
        P(None, TP),
        P(None, TP),
        P(),
        P(),
        P(TP, None),
        P(EP, TP, None, None),
        P(EP, TP, None),
        P(EP),
        P(),
        P(EP, None),
        P(EP, None),
        P(None, TP),
        P(None, TP),
        P(TP, None),
        P(ALL, None, None),
        P(ALL, None, None),
        P(ALL, None, None),
    )
    return jax.shard_map(
        body,
        mesh=split,
        in_specs=placed,
        out_specs=(P(EP, None), P(EP, TP, None)),
        check_vma=False,
    )
```
